32 devices in a mesh: gr: 2 (over x), fs: 4 (over z), tp: 4 (over y, core).
Axes of the slice: x: 2, y: 2, z: 4, core: 2. Of those that a mesh axis runs over, the one named last changes fastest.
Arguments:
- prompt: bfloat16 [4096, 2048], P(('gr', 'fs', 'tp')), may hold values from -6 to 6
- train_gate: float32 [16, 2048, 256], P(None, ('gr', 'fs'), 'tp'), may hold values from -0.125 to 0.125
- train_up: float32 [16, 2048, 256], P(None, ('gr', 'fs'), 'tp'), may hold values from -0.125 to 0.125
- train_down: float32 [16, 256, 2048], P(None, 'tp', ('gr', 'fs')), may hold values from -0.375 to 0.375
- train_shared_gate: float32 [2048, 256], P(('gr', 'fs'), 'tp'), may hold values from -0.125 to 0.125
- train_shared_up: float32 [2048, 256], P(('gr', 'fs'), 'tp'), may hold values from -0.125 to 0.125
- train_shared_down: float32 [256, 2048], P('tp', ('gr', 'fs')), may hold values from -0.375 to 0.375
- norm_gain: float32 [2048], P(('gr', 'fs')), may hold values from 0.1 to 1.9
- expert_ids: int32 [4096, 8], P(('gr', 'fs', 'tp')), may hold values from 0 to 15, all different within a row; in each aligned block of 128 rows (0 to 127, 128 to 255, ...) at most 65 rows name the same one
- route_weight: float32 [4096, 8], P(('gr', 'fs', 'tp')), may hold values from 0.05 to 0.6
Outputs:
- serve_gate: bfloat16 [16, 2048, 256], P(('fs', 'tp'))
- serve_up: bfloat16 [16, 2048, 256], P(('fs', 'tp'))
- serve_down: bfloat16 [16, 256, 2048], P(('fs', 'tp'))
- serve_shared_gate: bfloat16 [2048, 256], P(None, 'tp')
- serve_shared_up: bfloat16 [2048, 256], P(None, 'tp')
- serve_shared_down: bfloat16 [256, 2048], P('tp')
- mixed_out: bfloat16 [4096, 2048], P(('gr', 'fs', 'tp'))
The draws below stay inside these ranges and needn't reach their ends.
Inputs may be any that keep to these rules, and one draw needn't show every extreme that they name: `expert_ids`: each row names 8 different experts. Among the rows of one device no expert is named by more than 65 rows, and in some device's rows one expert is named by exactly 65.
All inputs are finite; a program needn't handle non-finite values.
Results may differ from the reference program's by a relative error of at most 0.012.
Values may be sent and summed in bfloat16 or wider, within the bound.
A program may use at most 128 MiB of HBM per device.

```python
import math
import jax
import jax.numpy as jnp
import numpy as np
from jax import lax

D = 2048
F = 256
SHARED = 256
TOP = 8
TOK_DEV = 128
EXPERTS = 16
SHARED_BLK = 64
CAP = 65
TOKENS = 4096
N_TP = 4


def steps_of(own_key, shape, shards, least, top_value):
    level, own = 1.0, jax.random.fold_in(own_key, 6)
    for position, shards_of in shards:
        heights = jnp.exp(jax.random.uniform(jax.random.fold_in(own, position), (shards_of,), jnp.float32, least / len(shards), top_value / len(shards)))
        level = level * jnp.repeat(heights, shape[position] // shards_of).reshape([-1 if axis == position else 1 for axis in range(len(shape))])
    return level


def shared_out(rng, own, number, rows, count, top, reach, lean):
    sequence = jax.random.permutation(rng, count)
    heavy_load, ordinary = load_shares(count, rows * top, reach, lean, True), load_shares(count, rows * top, reach, lean, False)
    places = jnp.arange(count)

    def named(sizes, turn):
        used = int((sizes > 0).sum())
        fixed = max(1, used // 4)
        shifted = fixed + (places - fixed + turn * (used - fixed)) % max(1, count - fixed)
        return jnp.zeros((count,), jnp.int32).at[sequence[jnp.where(places < fixed, places, shifted)]].set(jnp.asarray(sizes, jnp.int32))

    sizes = jnp.where(number % 4 == 0, named(heavy_load, number // 4), named(ordinary, number - number // 4 - 1))
    mixed = jax.random.permutation(jax.random.fold_in(own, 3), count)
    source_of, receiver = mixed[0:count // 2 * 2:2], mixed[1:count // 2 * 2:2]
    margin = jnp.minimum(sizes[source_of] - 1, reach - sizes[receiver]) // 2
    margin = jnp.where((source_of == sequence[0]) | (receiver == sequence[0]) | (sizes[receiver] == 0), 0, jnp.maximum(margin, 0))
    shifted = jax.random.randint(jax.random.fold_in(own, 4), (count // 2,), 0, 1 << 20) % (margin + 1)
    sizes = sizes.at[source_of].add(-shifted).at[receiver].add(shifted)
    items = jnp.searchsorted(jnp.cumsum(sizes), jnp.arange(rows * top), side="right").astype(jnp.int32)
    table = items.reshape(top, rows).T
    table = table[jax.random.permutation(jax.random.fold_in(own, 1), rows)]
    turn = jax.random.randint(jax.random.fold_in(own, 2), (rows, 1), 0, top)
    return jnp.take_along_axis(table, (jnp.arange(top)[None, :] + turn) % top, axis=1)


def load_shares(count, total, reach, skew, full):
    portions = [(1 << 20) // math.isqrt(rank ** skew) + 1 for rank in range(1, count + 1)]
    largest = reach if full else min(reach, max(-(-total // count), total * portions[0] // sum(portions)))
    least = 1 if total - largest >= count - 1 else 0
    given, rest = [largest] + [least] * (count - 1), total - largest - least * (count - 1)
    while rest > 0:
        free = [i for i in range(1, count) if given[i] < largest] or [i for i in range(1, count) if given[i] < reach]
        pool, remaining = sum([portions[i] for i in free]), rest
        for i in free:
            more = min(reach - given[i], max(1, remaining * portions[i] // pool), rest)
            given[i] = given[i] + more
            rest = rest - more
    return np.array(given)


def bell_draw(key, extent, deviation, reach, shards=(), kind=jnp.bfloat16):
    loudness = steps_of(key, extent, shards, -0.22, 0.18) if shards else 1.0
    array = jax.random.normal(key, extent, jnp.float32) * deviation * loudness
    return jnp.minimum(jnp.maximum(array, -reach), reach).astype(kind)


def setup_inputs(seed: int = 0) -> dict:
    keys = jax.random.split(jax.random.key(seed), 11)
    prompt = bell_draw(keys[0], (TOKENS, D), 1.0, 6.0, ((0, 32),))
    train_gate = bell_draw(keys[1], (EXPERTS, D, F), D ** -0.5, 0.125, ((1, 8), (2, 4)), jnp.float32)
    train_up = bell_draw(keys[2], (EXPERTS, D, F), D ** -0.5, 0.125, ((1, 8), (2, 4)), jnp.float32)
    train_down = bell_draw(keys[3], (EXPERTS, F, D), F ** -0.5, 0.375, ((1, 4), (2, 8)), jnp.float32)
    train_shared_gate = bell_draw(keys[4], (D, SHARED), D ** -0.5, 0.125, ((0, 8), (1, 4)), jnp.float32)
    train_shared_up = bell_draw(keys[5], (D, SHARED), D ** -0.5, 0.125, ((0, 8), (1, 4)), jnp.float32)
    train_shared_down = bell_draw(keys[6], (SHARED, D), SHARED ** -0.5, 0.375, ((0, 4), (1, 8)), jnp.float32)
    norm_gain = jnp.clip(1.0 + 0.18 * jax.random.normal(keys[7], (D,), jnp.float32), 0.1, 1.9)
    expert_ids_keys = jax.random.split(jax.random.fold_in(keys[8], 1), TOKENS // TOK_DEV)
    expert_ids_turns = jax.random.permutation(jax.random.fold_in(keys[8], 3), TOKENS // TOK_DEV)
    expert_ids = jax.vmap(lambda own, number: shared_out(jax.random.fold_in(keys[8], 2), own, number, TOK_DEV, EXPERTS, TOP, CAP, 1))(expert_ids_keys, expert_ids_turns).reshape((TOKENS, TOP))
    route_weight = jnp.clip(0.05 + 0.55 * jax.random.uniform(keys[9], (TOKENS, TOP), jnp.float32) ** steps_of(keys[9], (TOKENS, TOP), ((0, 32),), -0.2, 0.2), 0.05, 0.6)
    return {"prompt": prompt, "train_gate": train_gate, "train_up": train_up, "train_down": train_down, "train_shared_gate": train_shared_gate, "train_shared_up": train_shared_up, "train_shared_down": train_shared_down, "norm_gain": norm_gain, "expert_ids": expert_ids, "route_weight": route_weight}


eps_norm = 1e-06

def swiglu_rows(inputs, gate_w, up_w, down_w):
    gate_val = jnp.dot(inputs, gate_w, preferred_element_type=jnp.float32)
    up_val = jnp.dot(inputs, up_w, preferred_element_type=jnp.float32)
    hidden = (jax.nn.silu(gate_val) * up_val).astype(jnp.bfloat16)
    return jnp.dot(hidden, down_w, preferred_element_type=jnp.float32).astype(jnp.bfloat16)

def reference(prompt, train_gate, train_up, train_down, train_shared_gate, train_shared_up, train_shared_down, norm_gain, expert_ids, route_weight):
    gain_col = norm_gain[:, None]
    serve_gate = (train_gate * gain_col[None]).astype(jnp.bfloat16)
    serve_up = (train_up * gain_col[None]).astype(jnp.bfloat16)
    serve_down = train_down.astype(jnp.bfloat16)
    serve_shared_gate = (train_shared_gate * gain_col).astype(jnp.bfloat16)
    serve_shared_up = (train_shared_up * gain_col).astype(jnp.bfloat16)
    serve_shared_down = train_shared_down.astype(jnp.bfloat16)
    widened = prompt.astype(jnp.float32)
    normed = (widened * lax.rsqrt(lax.optimization_barrier(jnp.mean(widened * widened, axis=-1, keepdims=True)) + eps_norm)).astype(jnp.bfloat16)
    shared_act = (jax.nn.silu(jnp.dot(normed, serve_shared_gate, preferred_element_type=jnp.float32)) * jnp.dot(normed, serve_shared_up, preferred_element_type=jnp.float32)).astype(jnp.bfloat16)
    shared_sum = jnp.zeros((TOKENS, D), jnp.float32)
    for column in range(N_TP):
        first_row = column * SHARED_BLK
        partial_out = jnp.dot(shared_act[:, first_row:first_row + SHARED_BLK], serve_shared_down[first_row:first_row + SHARED_BLK], preferred_element_type=jnp.float32).astype(jnp.bfloat16)
        partial_out = lax.optimization_barrier(partial_out)
        shared_sum = shared_sum + partial_out.astype(jnp.float32)
    blocks = TOKENS // TOK_DEV
    flat_ids = expert_ids.reshape(blocks, TOK_DEV * TOP).astype(jnp.int32)
    onehot = (flat_ids[:, :, None] == jnp.arange(EXPERTS, dtype=jnp.int32)[None, None, :]).astype(jnp.int32)
    earlier = jnp.cumsum(onehot, axis=1) - onehot
    places = lax.optimization_barrier(jnp.sum(earlier * onehot, axis=-1)).astype(jnp.int32)
    block_ids = jnp.arange(blocks, dtype=jnp.int32)[:, None]
    token_ids = block_ids * TOK_DEV + jnp.arange(TOK_DEV * TOP, dtype=jnp.int32)[None, :] // TOP
    target = ((flat_ids * blocks + block_ids) * CAP + places).reshape(-1).astype(jnp.int32)
    row_table = jnp.full((EXPERTS * blocks * CAP,), TOKENS, jnp.int32).at[target].set(token_ids.reshape(-1).astype(jnp.int32)).reshape(EXPERTS, blocks * CAP)
    row_weights = jnp.zeros((EXPERTS * blocks * CAP,), jnp.float32).at[target].set(route_weight.reshape(-1)).reshape(EXPERTS, blocks * CAP)
    padded_rows = jnp.concatenate([normed, jnp.zeros((1, D), jnp.bfloat16)], axis=0)

    def add_expert(totals, expert_data):
        rows_index, weights_here, gate_w, up_w, down_w = expert_data
        outputs = swiglu_rows(padded_rows[rows_index], gate_w, up_w, down_w)
        return (totals.at[rows_index].add(weights_here[:, None] * outputs.astype(jnp.float32)), None)
    totals, _ = lax.scan(add_expert, jnp.zeros((TOKENS + 1, D), jnp.float32), (row_table, row_weights, serve_gate, serve_up, serve_down))
    mixed_out = (totals[:TOKENS] + shared_sum).astype(jnp.bfloat16)
    return (serve_gate, serve_up, serve_down, serve_shared_gate, serve_shared_up, serve_shared_down, mixed_out)
```

```python
import functools

import jax
import jax.numpy as jnp
from jax import lax
from jax.experimental import pallas as pl
from jax.experimental.pallas import tpu as pltpu
from jax.sharding import PartitionSpec as P

eps_norm = 1e-06
MESH = pl.DeviceIdType.MESH
CORES = 2
VMEM_PLAN = 40 * 2**20
VMEM_LIMIT = 60 * 2**20


def line_kernel(
    n_gr, n_fs, n_tp, parts,
    p_ref, gt_ref, ut_ref, dn_ref, sg_ref, su_ref, sd_ref, gain_ref, ids_ref, rw_ref,
    gate_hbm, up_hbm, down_hbm, sg_hbm, su_hbm, sd_hbm, mixed_out,
    x_all, t_all, e_in, w_all, s_in, s_all, q_all, gate_out, up_out, act, part, ru, rd,
    xr, tr, er, sr, fr, qr, ur, dr,
    zs, zd, xs, ys, xd, yd, fs_, ws, ss, sx, qs, us, ds_, loc, res_sem,
):
    gr, z, tp = lax.axis_index("gr"), lax.axis_index("fs"), lax.axis_index("tp")
    y, c = tp // CORES, tp % CORES
    sides = n_tp // CORES
    x_peer, y_other, c_other = 1 - gr, 1 - y, 1 - c
    _, hid, cols = s_in.shape
    sub, width = x_all.shape[2], x_all.shape[3]
    rows = parts * sub
    full = n_gr * n_fs
    quarter = hid // n_fs

    def dev(g, f, t):
        return {"gr": g, "fs": f, "tp": t}

    to_x, to_y = dev(x_peer, z, tp), dev(gr, z, y_other * CORES + c)
    to_c = dev(gr, z, y * CORES + c_other)
    up, down = dev(gr, z + 1, tp), dev(gr, z - 1, tp)
    has_up, has_down = z < n_fs - 1, z > 0

    barrier = pltpu.get_barrier_semaphore()

    def greet(where):
        pl.semaphore_signal(barrier, inc=1, device_id=where, device_id_type=MESH)

    for dz in range(n_fs):
        for dc in range(CORES):
            if dz or dc:
                greet(dev(gr, (z + dz) % n_fs, y * CORES + (c + dc) % CORES))
    greet(to_x)
    greet(to_y)

    gain = gain_ref[...]
    s_in[0] = (sg_ref[...] * gain).astype(jnp.bfloat16)
    s_in[1] = (su_ref[...] * gain).astype(jnp.bfloat16)
    s_in[2] = sd_ref[...].astype(jnp.bfloat16)

    def cast(i, carry):
        f, t = i // n_tp, i % n_tp
        e_in[f, t % CORES, t // CORES, 0] = (gt_ref[i] * gain).astype(jnp.bfloat16)
        e_in[f, t % CORES, t // CORES, 1] = (ut_ref[i] * gain).astype(jnp.bfloat16)
        e_in[f, t % CORES, t // CORES, 2] = dn_ref[i].astype(jnp.bfloat16)
        return carry

    lax.fori_loop(0, n_fs * n_tp, cast, 0)
    for h in range(parts):
        v = p_ref[h * sub : (h + 1) * sub, :].astype(jnp.float32)
        mean = jnp.mean(v * v, axis=-1, keepdims=True)
        x_all[z, h] = (v * lax.rsqrt(mean + eps_norm)).astype(jnp.bfloat16)
    shape = t_all.shape[1:]
    table = jnp.zeros(shape, jnp.float32)
    which = lax.broadcasted_iota(jnp.int32, shape, 0)
    for k in range(ids_ref.shape[0]):
        table = table + jnp.where(ids_ref[k : k + 1, :] == which, rw_ref[k : k + 1, :], 0.0)
    t_all[z] = table
    pl.semaphore_wait(barrier, n_fs * CORES + 1)

    def remote(src, dst, send, recv, where):
        return pltpu.make_async_remote_copy(
            src_ref=src, dst_ref=dst, send_sem=send, recv_sem=recv,
            device_id=where, device_id_type=MESH,
        )

    pending = []

    def go(cond, copies):
        pending.append((cond, copies))

        def start():
            for one in copies:
                one.start()

        if cond is None:
            start()
        else:
            pl.when(cond)(start)

    def slab(g, f, t, core):
        at = pl.ds(pl.multiple_of(t * hid, hid), hid)
        return w_all.at[g * n_fs + f, core, :, :, at, :]

    def got(g, f, t):
        return er.at[(g * n_fs + f) * n_tp + t]

    def send_expert(way, d):
        f = z + d if way == 0 else z - d
        there = f < n_fs if way == 0 else f >= 0
        for i in range(CORES):
            core = c if i == 0 else c_other
            go(there, [remote(
                e_in.at[f, core], slab(gr, z, tp, core), zs.at[way, d, i],
                got(gr, z, tp), dev(gr, f, y * CORES + core),
            )])

    def wait_slab(g, f, t):
        remote(e_in.at[0, 0], slab(g, f, t, c), zs.at[0, 0, 0], got(g, f, t), to_x).wait_recv()

    def pass_slab(g, f, t, sem, where, src=None):
        place = slab(g, f, t, c)
        return remote(place if src is None else src, place, sem, got(g, f, t), where)

    def row_copies(f, h, sem, where):
        copies = [remote(x_all.at[f, h], x_all.at[f, h], sem.at[h], xr.at[f, h], where)]
        if h == 0:
            copies.append(remote(t_all.at[f], t_all.at[f], sem.at[parts], tr.at[f], where))
        return copies

    def s_cols(g, f):
        return s_all.at[:, :, pl.ds(pl.multiple_of((g * n_fs + f) * cols, 128), cols)]

    def s_copy(src, g, f, sem, where):
        return remote(src, s_cols(g, f), sem, sr.at[g * n_fs + f], where)

    mine = e_in.at[z, c]
    own_k = gr * n_fs + z
    locals_ = [
        pltpu.make_async_copy(mine, slab(gr, z, tp, c), loc.at[0]),
        pltpu.make_async_copy(s_in, s_cols(gr, z), loc.at[1]),
    ]
    go(None, [remote(
        e_in.at[z, c_other], slab(gr, z, tp, c_other), zs.at[0, 0, 1], got(gr, z, tp), to_c
    )])
    go(None, [pass_slab(gr, z, tp, xs.at[z * CORES + c], to_x, mine)])
    go(None, [pass_slab(gr, z, tp, ys.at[z * CORES + c], to_y, mine)])
    send_expert(0, 1)
    send_expert(1, 1)
    for one in locals_:
        one.start()
    for h in range(parts):
        go(has_up, row_copies(z, h, zd.at[0, 0], up))
        go(has_down, row_copies(z, h, zd.at[1, 0], down))
    for d in range(2, n_fs):
        send_expert(0, d)
        send_expert(1, d)
    go(has_up, [s_copy(s_in, gr, z, ss.at[0, 0], up)])
    go(has_down, [s_copy(s_in, gr, z, ss.at[1, 0], down)])

    def reach(d):
        if d == 0:
            return [(0, z, None)]
        return [(0, z - d, z - d >= 0), (1, z + d, z + d < n_fs)]

    def when(cond, f):
        if cond is None:
            f()
        else:
            pl.when(cond)(f)

    def own_column(d):
        for _, f, there in reach(d):
            for i in range(CORES):
                if d == 0 and i == 0:
                    continue
                core = c if i == 0 else c_other
                t = y * CORES + core
                when(there, functools.partial(wait_slab, gr, f, t))
                go(there, [
                    pass_slab(gr, f, t, xs.at[f * CORES + core], to_x),
                    pass_slab(gr, f, t, ys.at[f * CORES + core], to_y),
                ])

    def give(g, f, there):
        k = g * n_fs + f
        go(there, [remote(w_all.at[k, c], w_all.at[k, c], fs_.at[k], fr.at[k], to_c)])

        def turn():
            at = pl.ds(pl.multiple_of(k * cols, 128), cols)
            gate_out[at, :] = w_all[k, c, y, 0].T
            up_out[at, :] = w_all[k, c, y, 1].T
            pltpu.make_async_copy(gate_out.at[at, :], gate_hbm.at[at, :], res_sem.at[0, k]).start()
            pltpu.make_async_copy(up_out.at[at, :], up_hbm.at[at, :], res_sem.at[1, k]).start()
            pltpu.make_async_copy(
                w_all.at[k, c, y, 2], down_hbm.at[:, at], res_sem.at[2, k]
            ).start()

        when(there, turn)

    def neighbours(d):
        for _, f, there in reach(d):
            for core in range(CORES):
                when(there, functools.partial(wait_slab, x_peer, f, y * CORES + core))
                if core == 0:
                    go(there, [pass_slab(x_peer, f, y * CORES, yd.at[f], to_y)])
                when(there, functools.partial(wait_slab, gr, f, y_other * CORES + core))
                if core == 1:
                    go(there, [pass_slab(gr, f, y_other * CORES + 1, xd.at[f], to_x)])
            if d == 0:
                locals_[0].wait()
            give(gr, f, there)

    def corners(d):
        for _, f, there in reach(d):
            for core in range(CORES):
                when(there, functools.partial(wait_slab, x_peer, f, y_other * CORES + core))
            give(x_peer, f, there)

    def line_rows(d):
        for h in range(parts):
            for way, f, there in reach(d):
                more = has_up if way == 0 else has_down
                onward = up if way == 0 else down

                def wait(f=f, h=h):
                    for one in row_copies(f, h, zd.at[0, 0], up):
                        one.wait_recv()

                when(there, wait)
                go(there & more, row_copies(f, h, zd.at[way, d], onward))

    def wait_shared(g, f):
        s_copy(s_in, g, f, sx.at[0], to_x).wait_recv()

    def line_shared(d):
        for way, f, there in reach(d):
            more = has_up if way == 0 else has_down
            onward = up if way == 0 else down
            if d:
                when(there, functools.partial(wait_shared, gr, f))
                go(there & more, [s_copy(s_cols(gr, f), gr, f, ss.at[way, d], onward)])
            go(there, [s_copy(s_in if d == 0 else s_cols(gr, f), gr, f, sx.at[f], to_x)])

    own_column(0)
    own_column(1)
    line_shared(0)
    neighbours(0)
    line_rows(1)
    line_shared(1)
    own_column(2)
    neighbours(1)
    line_rows(2)
    line_shared(2)
    own_column(3)
    neighbours(2)
    corners(0)
    line_rows(3)
    line_shared(3)
    locals_[1].wait()
    for f in range(n_fs):
        wait_shared(x_peer, f)

    piece = pl.ds(pl.multiple_of(z * quarter, quarter), quarter)

    def q_at(t):
        return q_all.at[:, pl.ds(pl.multiple_of(t * quarter, quarter), quarter), :]

    def q_copy(src, t, i, where):
        return remote(src, q_at(t), qs.at[i], qr.at[t], where)

    go(None, [q_copy(s_all.at[:, piece, :], tp, 0, to_y)])
    go(None, [q_copy(s_all.at[:, piece, :], tp, 1, to_c)])
    near_q = pltpu.make_async_copy(s_all.at[:, piece, :], q_at(tp), loc.at[2])
    near_q.start()
    t_y = y_other * CORES + c
    q_copy(q_at(t_y), t_y, 2, to_c).wait_recv()
    go(None, [q_copy(q_at(t_y), t_y, 2, to_c)])
    results = [
        pltpu.make_async_copy(s_all.at[i], dst, res_sem.at[3, i])
        for i, dst in enumerate((sg_hbm, su_hbm, sd_hbm))
    ]
    for one in results:
        one.start()
    neighbours(3)
    for d in range(1, n_fs):
        corners(d)
    near_q.wait()
    for side in range(sides):
        t = side * CORES + c_other
        q_copy(q_at(t), t, 2, to_c).wait_recv()
    for k in range(full):
        remote(w_all.at[k, c], w_all.at[k, c_other], fs_.at[k], fr.at[k], to_c).wait_recv()

    def wide(v):
        return v.astype(jnp.float32)

    def nt(a, b):
        return lax.dot_general(a, b, (((1,), (1,)), ((), ())), preferred_element_type=jnp.float32)

    def u_copy(t, h):
        return remote(part.at[t, h], ru.at[t, h], us.at[t, h], ur.at[t, h], up)

    def d_copy(t, h):
        return remote(part.at[t, h], rd.at[t, h], ds_.at[t, h], dr.at[t, h], down)

    def block(p, carry):
        falling = n_fs - 1 - p
        falling = jnp.where(falling <= z, falling - 1, falling)
        rising = jnp.where(p >= z, p + 1, p)
        t = jnp.where(p == n_fs - 1, z, jnp.where(z < n_fs // 2, falling, rising))
        xs_t = x_all[t].reshape(rows, width)
        both = nt(xs_t, q_all[0:2].reshape(2 * hid, width))
        extra = (jax.nn.silu(both[:, :hid]) * both[:, hid:]).astype(jnp.bfloat16)

        def expert(s, inner):
            core, side = s // sides, s % sides
            total = None
            for k in range(full):
                w = w_all[k, core, side, 0:2].reshape(2 * n_tp * hid, cols)
                one = nt(xs_t[:, k * cols : (k + 1) * cols], w)
                total = one if total is None else total + one
            e = z * n_tp + side * CORES + core
            scale = jnp.broadcast_to(t_all[t, pl.ds(e, 1), :], (rows, rows)).T[:, :1]
            val = jax.nn.silu(total[:, : n_tp * hid]) * total[:, n_tp * hid :] * scale
            act[s] = val.astype(jnp.bfloat16)
            return inner

        lax.fori_loop(0, n_tp, expert, 0)

        def columns(k, inner):
            at = pl.ds(pl.multiple_of(k * cols, 128), cols)
            total = jnp.dot(extra, q_all[2, :, at], preferred_element_type=jnp.float32)
            for s in range(n_tp):
                total = total + jnp.dot(
                    act[s], w_all[k, s // sides, s % sides, 2], preferred_element_type=jnp.float32
                )
            part[t, :, :, at] = total.astype(jnp.bfloat16).reshape(parts, sub, cols)
            return inner

        lax.fori_loop(0, full, columns, 0)
        for h in range(parts):
            pl.when((t > z) & jnp.logical_not(has_down))(lambda: u_copy(t, h).start())
            pl.when((t < z) & jnp.logical_not(has_up))(lambda: d_copy(t, h).start())
        return carry

    lax.fori_loop(0, n_fs, block, 0)

    for d in range(n_fs - 1, 0, -1):
        for h in range(parts):
            for way, there, before in (
                (0, z + d < n_fs, has_down),
                (1, z - d >= 0, has_up),
            ):
                t = z + d if way == 0 else z - d
                copy, arrived = (u_copy, ru) if way == 0 else (d_copy, rd)

                @pl.when(there & before)
                def _(t=t, h=h, copy=copy, arrived=arrived):
                    copy(t, h).wait_recv()
                    part[t, h] = (wide(part[t, h]) + wide(arrived[t, h])).astype(jnp.bfloat16)
                    copy(t, h).start()

    for h in range(parts):

        @pl.when(has_down & has_up)
        def _(h=h):
            u_copy(z, h).wait_recv()
            d_copy(z, h).wait_recv()
            mixed_out[h] = (
                wide(part[z, h]) + wide(ru[z, h]) + wide(rd[z, h])
            ).astype(jnp.bfloat16)

        @pl.when(jnp.logical_not(has_up))
        def _(h=h):
            u_copy(z, h).wait_recv()
            mixed_out[h] = (wide(part[z, h]) + wide(ru[z, h])).astype(jnp.bfloat16)

        @pl.when(jnp.logical_not(has_down))
        def _(h=h):
            d_copy(z, h).wait_recv()
            mixed_out[h] = (wide(part[z, h]) + wide(rd[z, h])).astype(jnp.bfloat16)

    for one in results:
        one.wait()
    for k in range(full):
        at = pl.ds(k * cols, cols)
        pltpu.make_async_copy(gate_out.at[at, :], gate_hbm.at[at, :], res_sem.at[0, k]).wait()
        pltpu.make_async_copy(up_out.at[at, :], up_hbm.at[at, :], res_sem.at[1, k]).wait()
        pltpu.make_async_copy(w_all.at[k, c, y, 2], down_hbm.at[:, at], res_sem.at[2, k]).wait()
    for cond, copies in pending:
        when(cond, lambda copies=copies: [one.wait_send() for one in copies] and None)
    for d in range(1, n_fs):
        for h in range(parts):
            pl.when(z + d < n_fs)(lambda d=d, h=h: u_copy(z + d, h).wait_send())
            pl.when(z - d >= 0)(lambda d=d, h=h: d_copy(z - d, h).wait_send())


def copy_kernel(count, *refs):
    ins, outs, bufs, sems = refs[:count], refs[count : 2 * count], refs[2 * count : -1], refs[-1]
    loads = [pltpu.make_async_copy(ins[i], bufs[i], sems.at[0, i]) for i in range(count)]
    stores = [pltpu.make_async_copy(bufs[i], outs[i], sems.at[1, i]) for i in range(count)]
    for one in loads:
        one.start()
    for one, then in zip(loads, stores):
        one.wait()
        then.start()
    for one in stores:
        one.wait()


def copied(arrays):
    count = len(arrays)
    return pl.pallas_call(
        functools.partial(copy_kernel, count),
        out_shape=tuple(jax.ShapeDtypeStruct(a.shape, a.dtype) for a in arrays),
        in_specs=[pl.BlockSpec(memory_space=pl.ANY)] * count,
        out_specs=(pl.BlockSpec(memory_space=pl.ANY),) * count,
        scratch_shapes=[pltpu.VMEM(a.shape, a.dtype) for a in arrays]
        + [pltpu.SemaphoreType.DMA((2, count))],
        compiler_params=pltpu.CompilerParams(vmem_limit_bytes=VMEM_LIMIT),
    )(*arrays)


def line_body(
    n_gr, n_fs, n_tp,
    prompt, train_gate, train_up, train_down, train_shared_gate, train_shared_up,
    train_shared_down, norm_gain, expert_ids, route_weight,
):
    experts, cols, hid = train_gate.shape
    rows, width = prompt.shape
    full, parts, sides = n_gr * n_fs, 2, n_tp // CORES
    sub, wide_hid = rows // parts, n_tp * hid
    bf16 = jnp.bfloat16
    vmem = pl.BlockSpec(memory_space=pltpu.VMEM)
    dma = pltpu.SemaphoreType.DMA
    shape = jax.ShapeDtypeStruct
    outs = pl.pallas_call(
        functools.partial(line_kernel, n_gr, n_fs, n_tp, parts),
        out_shape=(
            shape((width, wide_hid), bf16),
            shape((width, wide_hid), bf16),
            shape((wide_hid, width), bf16),
            shape((hid, width), bf16),
            shape((hid, width), bf16),
            shape((hid, width), bf16),
            shape((parts, sub, width), bf16),
        ),
        in_specs=[vmem] * 10,
        out_specs=(pl.BlockSpec(memory_space=pl.ANY),) * 6 + (vmem,),
        scratch_shapes=[
            pltpu.VMEM((n_fs, parts, sub, width), bf16),
            pltpu.VMEM((n_fs, experts, rows), jnp.float32),
            pltpu.VMEM((n_fs, CORES, sides, 3, hid, cols), bf16),
            pltpu.VMEM((full, CORES, sides, 3, wide_hid, cols), bf16),
            pltpu.VMEM((3, hid, cols), bf16),
            pltpu.VMEM((3, hid, width), bf16),
            pltpu.VMEM((3, hid, width), bf16),
            pltpu.VMEM((width, wide_hid), bf16),
            pltpu.VMEM((width, wide_hid), bf16),
            pltpu.VMEM((n_tp, rows, wide_hid), bf16),
            pltpu.VMEM((n_fs, parts, sub, width), bf16),
            pltpu.VMEM((n_fs, parts, sub, width), bf16),
            pltpu.VMEM((n_fs, parts, sub, width), bf16),
            dma((n_fs, parts)), dma((n_fs,)), dma((full * n_tp,)), dma((full,)), dma((full,)),
            dma((n_tp,)), dma((n_fs, parts)), dma((n_fs, parts)),
            dma((2, n_fs, CORES)), dma((2, n_fs, parts + 1)), dma((n_fs * CORES,)),
            dma((n_fs * CORES,)), dma((n_fs,)), dma((n_fs,)), dma((full,)), dma((1,)),
            dma((2, n_fs)), dma((n_fs,)), dma((3,)), dma((n_fs, parts)), dma((n_fs, parts)),
            dma((3,)), dma((4, full)),
        ],
        compiler_params=pltpu.CompilerParams(
            collective_id=0, has_side_effects=True, vmem_limit_bytes=VMEM_LIMIT
        ),
    )(
        prompt, train_gate.transpose(0, 2, 1), train_up.transpose(0, 2, 1), train_down,
        train_shared_gate.T, train_shared_up.T, train_shared_down, norm_gain[None, :],
        expert_ids.T, route_weight.T,
    )
    serve_gate, serve_up, serve_down, s_gate, s_up, s_down, mixed_out = copied(outs)
    return (
        serve_gate[None], serve_up[None], serve_down[None],
        s_gate.T, s_up.T, s_down, mixed_out.reshape(rows, width),
    )


def regroup(stacked, lowered):
    stacked = lax.all_to_all(
        lax.all_to_all(stacked, "fs", split_axis=0, concat_axis=2, tiled=True),
        "tp",
        split_axis=0,
        concat_axis=3,
        tiled=True,
    )
    lowered = lax.all_to_all(
        lax.all_to_all(lowered, "fs", split_axis=0, concat_axis=2, tiled=True),
        "tp",
        split_axis=0,
        concat_axis=1,
        tiled=True,
    )
    return (stacked, lowered)


def body(
    prompt,
    train_gate,
    train_up,
    train_down,
    train_shared_gate,
    train_shared_up,
    train_shared_down,
    norm_gain,
    expert_ids,
    route_weight,
):
    gain_col = norm_gain[:, None]
    stacked = jnp.stack((train_gate * gain_col[None], train_up * gain_col[None]), axis=1).astype(
        jnp.bfloat16
    )
    lowered = train_down.astype(jnp.bfloat16)
    stacked, lowered = regroup(stacked, lowered)
    stacked, lowered = (
        lax.all_gather(stacked, "gr", axis=2, tiled=True),
        lax.all_gather(lowered, "gr", axis=2, tiled=True),
    )
    serve_gate = stacked[:, 0]
    serve_up = stacked[:, 1]
    serve_shared_gate, serve_shared_up, serve_shared_down = (
        lax.all_gather(
            (train_shared_gate * gain_col).astype(jnp.bfloat16), ("gr", "fs"), axis=0, tiled=True
        ),
        lax.all_gather(
            (train_shared_up * gain_col).astype(jnp.bfloat16), ("gr", "fs"), axis=0, tiled=True
        ),
        lax.all_gather(train_shared_down.astype(jnp.bfloat16), ("gr", "fs"), axis=1, tiled=True),
    )
    widened = prompt.astype(jnp.float32)
    normed = (
        widened * lax.rsqrt(jnp.mean(widened * widened, axis=-1, keepdims=True) + eps_norm)
    ).astype(jnp.bfloat16)
    block_rows = lax.all_gather(normed, "tp", axis=0, tiled=True)
    gate_val = jnp.dot(block_rows, serve_shared_gate, preferred_element_type=jnp.float32)
    up_val = jnp.dot(block_rows, serve_shared_up, preferred_element_type=jnp.float32)
    shared_act = (jax.nn.silu(gate_val) * up_val).astype(jnp.bfloat16)
    shared_sum = lax.psum_scatter(
        jnp.dot(shared_act, serve_shared_down, preferred_element_type=jnp.float32).astype(
            jnp.bfloat16
        ),
        "tp",
        scatter_dimension=0,
        tiled=True,
    ).astype(jnp.float32)
    row_count = prompt.shape[0]
    top_count = expert_ids.shape[1]
    model_width = prompt.shape[1]
    expert_count = lax.axis_size("fs") * lax.axis_size("tp")
    capacity = row_count * top_count // expert_count + 1
    flat_ids = expert_ids.reshape(-1)
    onehot = (flat_ids[:, None] == jnp.arange(expert_count, dtype=jnp.int32)[None, :]).astype(
        jnp.int32
    )
    earlier = jnp.cumsum(onehot, axis=0) - onehot
    places = jnp.sum(earlier * onehot, axis=1)
    slot_ids = (flat_ids * capacity + places).reshape(row_count, top_count)
    slot_range = jnp.arange(expert_count * capacity, dtype=jnp.int32)
    dispatch = jnp.any(slot_range[:, None, None] == slot_ids[None, :, :], axis=-1).astype(
        jnp.bfloat16
    )
    outgoing = jnp.dot(dispatch, normed, preferred_element_type=jnp.float32).astype(jnp.bfloat16)
    outgoing = outgoing.reshape(expert_count, capacity, model_width)
    arrived = lax.all_to_all(outgoing, ("fs", "tp"), split_axis=0, concat_axis=0, tiled=True)
    source_count, slot_count, width_here = arrived.shape
    arrived_rows = arrived.reshape(source_count * slot_count, width_here)
    gate_val = jnp.dot(arrived_rows, serve_gate[0], preferred_element_type=jnp.float32)
    up_val = jnp.dot(arrived_rows, serve_up[0], preferred_element_type=jnp.float32)
    hidden = (jax.nn.silu(gate_val) * up_val).astype(jnp.bfloat16)
    result = jnp.dot(hidden, lowered[0], preferred_element_type=jnp.float32).astype(jnp.bfloat16)
    result = result.reshape(source_count, slot_count, width_here)
    returned = lax.all_to_all(result, ("fs", "tp"), split_axis=0, concat_axis=0, tiled=True)
    picked = returned.reshape(expert_count * capacity, model_width)[slot_ids]
    routed = jnp.sum(route_weight[:, :, None] * picked.astype(jnp.float32), axis=1)
    mixed_out = (routed + shared_sum).astype(jnp.bfloat16)
    return (
        serve_gate,
        serve_up,
        lowered,
        serve_shared_gate,
        serve_shared_up,
        serve_shared_down,
        mixed_out,
    )


def solution(mesh):
    placed = (
        P(("gr", "fs", "tp"), None),
        P(None, ("gr", "fs"), "tp"),
        P(None, ("gr", "fs"), "tp"),
        P(None, "tp", ("gr", "fs")),
        P(("gr", "fs"), "tp"),
        P(("gr", "fs"), "tp"),
        P("tp", ("gr", "fs")),
        P(("gr", "fs")),
        P(("gr", "fs", "tp"), None),
        P(("gr", "fs", "tp"), None),
    )
    n_gr, n_fs, n_tp = (mesh.shape[name] for name in ("gr", "fs", "tp"))

    def chosen(prompt, train_gate, *rest):
        rows, width = prompt.shape
        experts, cols, hid = train_gate.shape
        held = n_fs * n_tp * n_gr * CORES * 3 * hid * cols * 4 + 4 * n_fs * prompt.size * 2
        fits = n_gr == 2 and n_tp == 2 * CORES and n_fs % 2 == 0 and held < VMEM_PLAN
        even = experts == n_fs * n_tp and cols * n_gr * n_fs == width and rows == 128
        if fits and even and hid % (16 * n_fs) == 0 and cols % 128 == 0:
            return line_body(n_gr, n_fs, n_tp, prompt, train_gate, *rest)
        return body(prompt, train_gate, *rest)

    return jax.shard_map(
        chosen,
        mesh=mesh,
        in_specs=placed,
        out_specs=(
            P(("fs", "tp"), None, None),
            P(("fs", "tp"), None, None),
            P(("fs", "tp"), None, None),
            P(None, "tp"),
            P(None, "tp"),
            P("tp", None),
            P(("gr", "fs", "tp"), None),
        ),
        check_vma=False,
    )
```

```python
import functools

import jax
import jax.numpy as jnp
from jax import lax
from jax.experimental import pallas as pl
from jax.experimental.pallas import tpu as pltpu
from jax.sharding import PartitionSpec as P

eps_norm = 1e-06
MESH = pl.DeviceIdType.MESH
CORES = 2
VMEM_PLAN = 40 * 2**20
VMEM_LIMIT = 60 * 2**20


def line_kernel(
    n_gr, n_fs, n_tp, parts,
    p_hbm, gt_hbm, ut_hbm, dn_hbm, tsg_hbm, tsu_hbm, tsd_hbm, gain_hbm, ids_hbm, rw_hbm,
    gate_hbm, up_hbm, down_hbm, sg_hbm, su_hbm, sd_hbm, mixed_hbm,
    p_ref, gt_ref, ut_ref, dn_ref, sg_ref, su_ref, sd_ref, gain_ref, ids_ref, rw_ref,
    x_all, t_all, e_in, w_all, s_in, s_all, gate_out, up_out, acc, act, base, mixed_out,
    part, ru, rd,
    xr, tr, er, sr, sc, fr, ur, dr,
    zs, zd, xs, ys, xd, yd, fs_, ss, sx, sy, sd, us, ds_, loc, res_sem, in_sem,
):
    gr, z, tp = lax.axis_index("gr"), lax.axis_index("fs"), lax.axis_index("tp")
    y, c = tp // CORES, tp % CORES
    sides = n_tp // CORES
    x_peer, y_other, c_other = 1 - gr, 1 - y, 1 - c
    _, hid, cols = s_in.shape
    sub, width = x_all.shape[2], x_all.shape[3]
    rows = parts * sub
    full = n_gr * n_fs
    wide_hid = n_tp * hid

    def dev(g, f, t):
        return {"gr": g, "fs": f, "tp": t}

    to_x, to_y = dev(x_peer, z, tp), dev(gr, z, y_other * CORES + c)
    to_c = dev(gr, z, y * CORES + c_other)
    up, down = dev(gr, z + 1, tp), dev(gr, z - 1, tp)
    has_up, has_down = z < n_fs - 1, z > 0
    inner = has_up & has_down
    outer = jnp.logical_not(inner)

    def far(p):
        if p == n_fs - 1:
            return z
        fall, rise = n_fs - 1 - p, p
        fall = jnp.where(fall <= z, fall - 1, fall)
        rise = jnp.where(rise >= z, rise + 1, rise)
        return jnp.where(z < n_fs // 2, fall, rise)

    order = [far(n_fs - 1 - p) for p in range(n_fs)]

    def place(f, at):
        rise = jnp.where(f < at, f + 1, f)
        fall = jnp.where(f > at, n_fs - f, n_fs - 1 - f)
        return jnp.where(f == at, 0, jnp.where(at < n_fs // 2, rise, fall))

    ins = [
        pltpu.make_async_copy(src, dst, in_sem.at[i])
        for i, (src, dst) in enumerate((
            (gain_hbm, gain_ref), (gt_hbm, gt_ref), (ut_hbm, ut_ref), (dn_hbm, dn_ref),
            (tsg_hbm, sg_ref), (tsu_hbm, su_ref), (tsd_hbm, sd_ref), (p_hbm, p_ref),
            (ids_hbm, ids_ref), (rw_hbm, rw_ref),
        ))
    ]
    for one in ins:
        one.start()

    barrier = pltpu.get_barrier_semaphore()

    def greet(where):
        pl.semaphore_signal(barrier, inc=1, device_id=where, device_id_type=MESH)

    for dz in range(n_fs):
        for dc in range(CORES):
            if dz or dc:
                greet(dev(gr, (z + dz) % n_fs, y * CORES + (c + dc) % CORES))
    greet(to_x)
    greet(to_y)

    for one in ins[:4]:
        one.wait()
    gain = gain_ref[...]

    def cast(i, carry):
        f, t = i // n_tp, i % n_tp
        e_in[f, t % CORES, t // CORES, 0] = (gt_ref[i] * gain).astype(jnp.bfloat16)
        e_in[f, t % CORES, t // CORES, 1] = (ut_ref[i] * gain).astype(jnp.bfloat16)
        e_in[f, t % CORES, t // CORES, 2] = dn_ref[i].astype(jnp.bfloat16)
        return carry

    lax.fori_loop(0, n_fs * n_tp, cast, 0)
    pl.semaphore_wait(barrier, n_fs * CORES + 1)

    def remote(src, dst, send, recv, where):
        return pltpu.make_async_remote_copy(
            src_ref=src, dst_ref=dst, send_sem=send, recv_sem=recv,
            device_id=where, device_id_type=MESH,
        )

    pending = []

    def when(cond, f):
        if cond is None:
            f()
        else:
            pl.when(cond)(f)

    def go(cond, copies):
        pending.append((cond, copies))

        def start():
            for one in copies:
                one.start()

        when(cond, start)

    def slab(g, f, t, core):
        at = pl.ds(pl.multiple_of(t * hid, hid), hid)
        return w_all.at[g * n_fs + f, core, :, :, at, :]

    def got(g, f, t):
        return er.at[(g * n_fs + f) * n_tp + t]

    def send_expert(d, i):
        core = c if i == 0 else c_other
        for way in (0, 1):
            f = z + d if way == 0 else z - d
            there = f < n_fs if way == 0 else f >= 0
            go(there, [remote(
                e_in.at[f, core], slab(gr, z, tp, core), zs.at[way, d, i],
                got(gr, z, tp), dev(gr, f, y * CORES + core),
            )])

    def wait_slab(g, f, t):
        remote(e_in.at[0, 0], slab(g, f, t, c), zs.at[0, 0, 0], got(g, f, t), to_x).wait_recv()

    def pass_slab(g, f, t, sem, where, src=None):
        place = slab(g, f, t, c)
        return remote(place if src is None else src, place, sem, got(g, f, t), where)

    def row_copies(f, h, sem, way):
        to = z + 1 if way == 0 else z - 1
        here, there = place(f, z), place(f, to)
        where = dev(gr, to, tp)
        copies = [remote(x_all.at[here, h], x_all.at[there, h], sem.at[h], xr.at[f, h], where)]
        if h == 0:
            copies.append(remote(t_all.at[f], t_all.at[f], sem.at[parts], tr.at[f], where))
        return copies

    def s_slab(g, f, t):
        lanes = pl.ds(pl.multiple_of((g * n_fs + f) * cols, 128), cols)
        return s_all.at[:, pl.ds(pl.multiple_of(t * hid, hid), hid), lanes]

    def s_copy(src, g, f, sem, where, t=tp):
        src = s_slab(g, f, t) if src is None else src
        return remote(src, s_slab(g, f, t), sem, sr.at[(g * n_fs + f) * n_tp + t], where)

    mine = e_in.at[z, c]
    go(None, [remote(
        e_in.at[z, c_other], slab(gr, z, tp, c_other), zs.at[0, 0, 1], got(gr, z, tp), to_c
    )])
    go(None, [pass_slab(gr, z, tp, xs.at[z * CORES + c], to_x, mine)])
    go(None, [pass_slab(gr, z, tp, ys.at[z * CORES + c], to_y, mine)])
    for i in range(CORES):
        for d in range(1, n_fs):
            send_expert(d, i)
    near_slab = pltpu.make_async_copy(mine, slab(gr, z, tp, c), loc.at[0])
    near_slab.start()

    for one in ins[4:]:
        one.wait()
    s_in[0] = (sg_ref[...] * gain).astype(jnp.bfloat16)
    s_in[1] = (su_ref[...] * gain).astype(jnp.bfloat16)
    s_in[2] = sd_ref[...].astype(jnp.bfloat16)
    for h in range(parts):
        v = p_ref[h * sub : (h + 1) * sub, :].astype(jnp.float32)
        mean = jnp.mean(v * v, axis=-1, keepdims=True)
        x_all[0, h] = (v * lax.rsqrt(mean + eps_norm)).astype(jnp.bfloat16)
    shape = t_all.shape[1:]
    table = jnp.zeros(shape, jnp.float32)
    which = lax.broadcasted_iota(jnp.int32, shape, 0)
    for k in range(ids_ref.shape[0]):
        table = table + jnp.where(ids_ref[k : k + 1, :] == which, rw_ref[k : k + 1, :], 0.0)
    t_all[z] = table

    near_s = pltpu.make_async_copy(s_in, s_slab(gr, z, tp), loc.at[1])
    near_s.start()

    def send_own(cond):
        for h in range(parts):
            for way in (0, 1):
                there = has_up if way == 0 else has_down
                go(there & cond, row_copies(z, h, zd.at[way], way))
        go(has_up & cond, [s_copy(s_in, gr, z, ss.at[0], up)])
        go(has_down & cond, [s_copy(s_in, gr, z, ss.at[1], down)])

    send_own(True)

    def own(p, i):
        f = order[p]
        core = c if i == 0 else c_other
        t = y * CORES + core
        wait_slab(gr, f, t)
        go(None, [pass_slab(gr, f, t, xs.at[f * CORES + core], to_x)])
        go(None, [pass_slab(gr, f, t, ys.at[f * CORES + core], to_y)])

    def result_copies(k):
        at = pl.ds(pl.multiple_of(k * cols, 128), cols)
        return [
            pltpu.make_async_copy(gate_out.at[at, :], gate_hbm.at[at, :], res_sem.at[0, k]),
            pltpu.make_async_copy(up_out.at[at, :], up_hbm.at[at, :], res_sem.at[1, k]),
            pltpu.make_async_copy(w_all.at[k, c, y, 2], down_hbm.at[:, at], res_sem.at[2, k]),
        ]

    def give(g, f):
        k = g * n_fs + f
        go(None, [remote(w_all.at[k, c], w_all.at[k, c], fs_.at[k], fr.at[k], to_c)])
        at = pl.ds(pl.multiple_of(k * cols, 128), cols)
        gate_out[at, :] = w_all[k, c, y, 0].T
        up_out[at, :] = w_all[k, c, y, 1].T
        for one in result_copies(k):
            one.start()

    def side(p, core):
        f = order[p]
        wait_slab(x_peer, f, y * CORES + core)
        if core == 0:
            go(None, [pass_slab(x_peer, f, y * CORES, yd.at[f], to_y)])
        wait_slab(gr, f, y_other * CORES + core)
        if core == 1:
            go(None, [pass_slab(gr, f, y_other * CORES + 1, xd.at[f], to_x)])

    def column(p):
        if p == 0:
            near_slab.wait()
        give(gr, order[p])

    def corner(p):
        f = order[p]
        for core in range(CORES):
            wait_slab(x_peer, f, y_other * CORES + core)
        give(x_peer, f)

    def row_part(p, h, most=None):
        f = order[p]

        def arrive():
            remote(x_all.at[p, h], x_all.at[p, h], zd.at[0, 0], xr.at[f, h], to_x).wait_recv()
            if h == 0:
                remote(t_all.at[f], t_all.at[f], zd.at[0, 0], tr.at[f], to_x).wait_recv()

        when(most, arrive)
        if most is inner:
            go((f < z) & inner, row_copies(f, h, zd.at[1 + p], 0))
            go((f > z) & inner, row_copies(f, h, zd.at[n_fs + p], 1))

    def wait_shared(g, f, t):
        s_copy(None, g, f, sx.at[0], to_x, t).wait_recv()

    def shared(p, most=True):
        f = order[p]
        src = None if p else s_in
        if p:
            when(None if most is True else most, functools.partial(wait_shared, gr, f, tp))
            go((f < z) & has_up & most, [s_copy(src, gr, f, ss.at[1 + p], up)])
            go((f > z) & has_down & most, [s_copy(src, gr, f, ss.at[n_fs + p], down)])
        most = None if most is True else most
        go(most, [s_copy(src, gr, f, sx.at[f], to_x)])
        go(most, [s_copy(src, gr, f, sy.at[gr * n_fs + f], to_y)])

    def shared_x(p):
        f = order[p]
        wait_shared(x_peer, f, tp)
        go(None, [s_copy(None, x_peer, f, sy.at[x_peer * n_fs + f], to_y)])

    def nt(a, b):
        return lax.dot_general(a, b, (((1,), (1,)), ((), ())), preferred_element_type=jnp.float32)

    def step(g, f, first=False):
        k = g * n_fs + f
        remote(w_all.at[k, c], w_all.at[k, c_other], fs_.at[k], fr.at[k], to_c).wait_recv()
        at = pl.ds(pl.multiple_of(k * cols, 128), cols)
        some = (n_fs - 1) * rows
        lhs = x_all[0 : n_fs - 1, :, :, at].reshape(some, cols)
        for s in range(n_tp):
            w = w_all[k, s // sides, s % sides, 0:2].reshape(2 * wide_hid, cols)
            val = nt(lhs, w)
            acc[s, 0:some] = val if first else acc[s, 0:some] + val

    def late():
        lhs = x_all[n_fs - 1].reshape(rows, width)

        def one(s, carry):
            total = None
            for k in range(full):
                w = w_all[k, s // sides, s % sides, 0:2].reshape(2 * wide_hid, cols)
                val = nt(lhs[:, k * cols : (k + 1) * cols], w)
                total = val if total is None else total + val
            acc[s, (n_fs - 1) * rows :] = total
            return carry

        lax.fori_loop(0, n_tp, one, 0)

    def s_slice(t):
        return s_all.at[:, pl.ds(pl.multiple_of(t * hid, hid), hid), :]

    def s_whole(t, i):
        return remote(s_slice(t), s_slice(t), sd.at[i], sc.at[t], to_c)

    s_results = [
        pltpu.make_async_copy(s_slice(tp).at[i], dst, res_sem.at[3, i])
        for i, dst in enumerate((sg_hbm, su_hbm, sd_hbm))
    ]
    t_y = y_other * CORES + c

    def shared_give():
        near_s.wait()
        go(None, [s_whole(tp, 0)])
        for one in s_results:
            one.start()
        for g in range(n_gr):
            for f in range(n_fs):
                wait_shared(g, f, t_y)
        go(None, [s_whole(t_y, 1)])

    def shared_act():
        for side in range(sides):
            s_whole(side * CORES + c_other, 0).wait_recv()
        lhs = x_all[0].reshape(rows, width)
        both = nt(lhs, s_all[0:2].reshape(2 * wide_hid, width))
        act[0] = (jax.nn.silu(both[:, :wide_hid]) * both[:, wide_hid:]).astype(jnp.bfloat16)

        def columns(k, inner):
            at = pl.ds(pl.multiple_of(k * cols, 128), cols)
            val = jnp.dot(act[0], s_all[2, :, at], preferred_element_type=jnp.float32)
            base[:, at] = val
            return inner

        lax.fori_loop(0, full, columns, 0)

    stages = []

    def then(f, *args):
        stages.append((f, args))

    def wide(v):
        return v.astype(jnp.float32)

    def u_copy(t, h):
        return remote(part.at[t, h], ru.at[t, h], us.at[t, h], ur.at[t, h], up)

    def d_copy(t, h):
        return remote(part.at[t, h], rd.at[t, h], ds_.at[t, h], dr.at[t, h], down)

    def when_way(t, ahead, behind):
        pl.when(t > z)(ahead)
        pl.when(t < z)(behind)

    def block(p):
        t = order[p]
        here = slice(p * rows, (p + 1) * rows)

        for s in range(n_tp):
            e = z * n_tp + (s % sides) * CORES + s // sides
            scale = jnp.broadcast_to(t_all[t, pl.ds(e, 1), :], (rows, rows)).T[:, :1]
            val = acc[s, here, :]
            val = jax.nn.silu(val[:, :wide_hid]) * val[:, wide_hid:] * scale
            act[s] = val.astype(jnp.bfloat16)

        group = 4

        def columns(j, carry):
            for i in range(group):
                k = j * group + i
                at = pl.ds(pl.multiple_of(k * cols, 128), cols)
                total = None
                for s in range(n_tp):
                    val = jnp.dot(
                        act[s], w_all[k, s // sides, s % sides, 2],
                        preferred_element_type=jnp.float32,
                    )
                    total = val if total is None else total + val
                part[t, :, :, at] = total.astype(jnp.bfloat16).reshape(parts, sub, cols)
            return carry

        lax.fori_loop(0, full // group, columns, 0)
        if p:
            for h in range(parts):
                pl.when((t > z) & jnp.logical_not(has_down))(lambda: u_copy(t, h).start())
                pl.when((t < z) & jnp.logical_not(has_up))(lambda: d_copy(t, h).start())

    def chain(p):
        t = order[p]
        for h in range(parts):
            for copy, arrived, cond in (
                (u_copy, ru, (t > z) & has_down), (d_copy, rd, (t < z) & has_up)
            ):

                @pl.when(cond)
                def _(h=h, copy=copy, arrived=arrived):
                    with jax.named_scope("chain"):
                        copy(t, h).wait_recv()
                    part[t, h] = (wide(part[t, h]) + wide(arrived[t, h])).astype(jnp.bfloat16)
                    copy(t, h).start()

    def mixed_copy(h):
        return pltpu.make_async_copy(mixed_out.at[h], mixed_hbm.at[h], loc.at[2 + h])

    def finish(h):
        mine_h = slice(h * sub, (h + 1) * sub)

        def total(*arrived):
            val = wide(part[z, h]) + base[mine_h, :]
            for one in arrived:
                val = val + wide(one)
            mixed_out[h] = val.astype(jnp.bfloat16)

        @pl.when(has_down & has_up)
        def _():
            u_copy(z, h).wait_recv()
            d_copy(z, h).wait_recv()
            total(ru[z, h], rd[z, h])

        @pl.when(jnp.logical_not(has_up))
        def _():
            u_copy(z, h).wait_recv()
            total(ru[z, h])

        @pl.when(jnp.logical_not(has_down))
        def _():
            d_copy(z, h).wait_recv()
            total(rd[z, h])

        mixed_copy(h).start()

    last = n_fs - 1
    then(own, 0, 1)
    for i in range(CORES):
        for p in range(1, n_fs):
            then(own, p, i)
            if i == 0 and p == last:
                then(side, 0, 0)
                then(side, 0, 1)
                then(column, 0)
    for p in range(1, last):
        then(side, p, 0)
        then(side, p, 1)
        then(column, p)
    for h in range(parts):
        for p in range(1, last):
            then(row_part, p, h, inner)
    then(corner, 0)
    then(side, last, 0)
    then(side, last, 1)
    then(column, last)
    then(shared, 0)
    for p in range(1, last):
        for h in range(parts):
            then(row_part, p, h, outer)
        then(shared, p, inner)
    then(corner, 1)
    for p in range(n_fs):
        then(step, gr, order[p], p == 0)
    for p in range(2):
        then(step, x_peer, order[p])
    then(shared, 1, outer)
    for p in range(2, n_fs):
        then(row_part, last, p - 2, inner)
        then(corner, p)
        then(step, x_peer, order[p])
    then(block, last - 1)
    then(shared, last, inner)
    for h in range(parts):
        then(row_part, last, h, outer)
    then(late)
    then(block, last)
    for p in range(1, last - 1):
        then(block, p)
    for p in range(2, n_fs):
        then(shared, p, outer)
    then(block, 0)
    then(chain, last - 1)
    for p in range(n_fs):
        then(shared_x, p)
    then(chain, last)
    then(shared_give)
    then(shared_act)
    for p in range(1, last - 1):
        then(chain, p)
    for h in range(parts):
        then(finish, h)

    for f, args in stages:
        with jax.named_scope(f.__name__ + "_".join(str(a) for a in args if type(a) is int)):
            f(*args)

    with jax.named_scope("drain"):
        for h in range(parts):
            mixed_copy(h).wait()
        for one in s_results:
            one.wait()
        for k in range(full):
            for one in result_copies(k):
                one.wait()
        for cond, copies in pending:
            when(cond, lambda copies=copies: [one.wait_send() for one in copies] and None)
        for d in range(1, n_fs):
            for h in range(parts):
                pl.when(z + d < n_fs)(lambda d=d, h=h: u_copy(z + d, h).wait_send())
                pl.when(z - d >= 0)(lambda d=d, h=h: d_copy(z - d, h).wait_send())


def copy_kernel(count, *refs):
    ins, outs, bufs, sems = refs[:count], refs[count : 2 * count], refs[2 * count : -1], refs[-1]
    loads = [pltpu.make_async_copy(ins[i], bufs[i], sems.at[0, i]) for i in range(count)]
    stores = [pltpu.make_async_copy(bufs[i], outs[i], sems.at[1, i]) for i in range(count)]
    for one in loads:
        one.start()
    for one, then in zip(loads, stores):
        one.wait()
        then.start()
    for one in stores:
        one.wait()


def copied(arrays):
    count = len(arrays)
    return pl.pallas_call(
        functools.partial(copy_kernel, count),
        out_shape=tuple(jax.ShapeDtypeStruct(a.shape, a.dtype) for a in arrays),
        in_specs=[pl.BlockSpec(memory_space=pl.ANY)] * count,
        out_specs=(pl.BlockSpec(memory_space=pl.ANY),) * count,
        scratch_shapes=[pltpu.VMEM(a.shape, a.dtype) for a in arrays]
        + [pltpu.SemaphoreType.DMA((2, count))],
        compiler_params=pltpu.CompilerParams(vmem_limit_bytes=VMEM_LIMIT),
    )(*arrays)


def line_body(
    n_gr, n_fs, n_tp,
    prompt, train_gate, train_up, train_down, train_shared_gate, train_shared_up,
    train_shared_down, norm_gain, expert_ids, route_weight,
):
    experts, cols, hid = train_gate.shape
    rows, width = prompt.shape
    full, parts, sides = n_gr * n_fs, 2, n_tp // CORES
    sub, wide_hid = rows // parts, n_tp * hid
    bf16 = jnp.bfloat16
    f32 = jnp.float32
    hbm = pl.BlockSpec(memory_space=pl.ANY)
    dma = pltpu.SemaphoreType.DMA
    shape = jax.ShapeDtypeStruct
    outs = pl.pallas_call(
        functools.partial(line_kernel, n_gr, n_fs, n_tp, parts),
        out_shape=(
            shape((width, wide_hid), bf16),
            shape((width, wide_hid), bf16),
            shape((wide_hid, width), bf16),
            shape((hid, width), bf16),
            shape((hid, width), bf16),
            shape((hid, width), bf16),
            shape((parts, sub, width), bf16),
        ),
        in_specs=[hbm] * 10,
        out_specs=(hbm,) * 7,
        scratch_shapes=[
            pltpu.VMEM((rows, width), bf16),
            pltpu.VMEM((experts, hid, cols), f32),
            pltpu.VMEM((experts, hid, cols), f32),
            pltpu.VMEM((experts, hid, cols), f32),
            pltpu.VMEM((hid, cols), f32),
            pltpu.VMEM((hid, cols), f32),
            pltpu.VMEM((hid, cols), f32),
            pltpu.VMEM((1, cols), f32),
            pltpu.VMEM((expert_ids.shape[1], rows), jnp.int32),
            pltpu.VMEM((expert_ids.shape[1], rows), f32),
            pltpu.VMEM((n_fs, parts, sub, width), bf16),
            pltpu.VMEM((n_fs, experts, rows), f32),
            pltpu.VMEM((n_fs, CORES, sides, 3, hid, cols), bf16),
            pltpu.VMEM((full, CORES, sides, 3, wide_hid, cols), bf16),
            pltpu.VMEM((3, hid, cols), bf16),
            pltpu.VMEM((3, wide_hid, width), bf16),
            pltpu.VMEM((width, wide_hid), bf16),
            pltpu.VMEM((width, wide_hid), bf16),
            pltpu.VMEM((n_tp, n_fs * rows, 2 * wide_hid), f32),
            pltpu.VMEM((n_tp, rows, wide_hid), bf16),
            pltpu.VMEM((rows, width), f32),
            pltpu.VMEM((parts, sub, width), bf16),
            pltpu.VMEM((n_fs, parts, sub, width), bf16),
            pltpu.VMEM((n_fs, parts, sub, width), bf16),
            pltpu.VMEM((n_fs, parts, sub, width), bf16),
            dma((n_fs, parts)), dma((n_fs,)), dma((full * n_tp,)), dma((full * n_tp,)),
            dma((n_tp,)), dma((full,)), dma((n_fs, parts)), dma((n_fs, parts)),
            dma((2, n_fs, CORES)), dma((2 * n_fs, parts + 1)), dma((n_fs * CORES,)),
            dma((n_fs * CORES,)), dma((n_fs,)), dma((n_fs,)), dma((full,)),
            dma((2 * n_fs,)), dma((n_fs,)), dma((full,)), dma((2,)),
            dma((n_fs, parts)), dma((n_fs, parts)),
            dma((2 + parts,)), dma((4, full)), dma((10,)),
        ],
        compiler_params=pltpu.CompilerParams(
            collective_id=0, has_side_effects=True, vmem_limit_bytes=VMEM_LIMIT
        ),
    )(
        prompt, train_gate.transpose(0, 2, 1), train_up.transpose(0, 2, 1), train_down,
        train_shared_gate.T, train_shared_up.T, train_shared_down, norm_gain[None, :],
        expert_ids.T, route_weight.T,
    )
    serve_gate, serve_up, serve_down, s_gate, s_up, s_down, mixed_out = copied(outs)
    return (
        serve_gate[None], serve_up[None], serve_down[None],
        s_gate.T, s_up.T, s_down, mixed_out.reshape(rows, width),
    )


def regroup(stacked, lowered):
    stacked = lax.all_to_all(
        lax.all_to_all(stacked, "fs", split_axis=0, concat_axis=2, tiled=True),
        "tp",
        split_axis=0,
        concat_axis=3,
        tiled=True,
    )
    lowered = lax.all_to_all(
        lax.all_to_all(lowered, "fs", split_axis=0, concat_axis=2, tiled=True),
        "tp",
        split_axis=0,
        concat_axis=1,
        tiled=True,
    )
    return (stacked, lowered)


def body(
    prompt,
    train_gate,
    train_up,
    train_down,
    train_shared_gate,
    train_shared_up,
    train_shared_down,
    norm_gain,
    expert_ids,
    route_weight,
):
    gain_col = norm_gain[:, None]
    stacked = jnp.stack((train_gate * gain_col[None], train_up * gain_col[None]), axis=1).astype(
        jnp.bfloat16
    )
    lowered = train_down.astype(jnp.bfloat16)
    stacked, lowered = regroup(stacked, lowered)
    stacked, lowered = (
        lax.all_gather(stacked, "gr", axis=2, tiled=True),
        lax.all_gather(lowered, "gr", axis=2, tiled=True),
    )
    serve_gate = stacked[:, 0]
    serve_up = stacked[:, 1]
    serve_shared_gate, serve_shared_up, serve_shared_down = (
        lax.all_gather(
            (train_shared_gate * gain_col).astype(jnp.bfloat16), ("gr", "fs"), axis=0, tiled=True
        ),
        lax.all_gather(
            (train_shared_up * gain_col).astype(jnp.bfloat16), ("gr", "fs"), axis=0, tiled=True
        ),
        lax.all_gather(train_shared_down.astype(jnp.bfloat16), ("gr", "fs"), axis=1, tiled=True),
    )
    widened = prompt.astype(jnp.float32)
    normed = (
        widened * lax.rsqrt(jnp.mean(widened * widened, axis=-1, keepdims=True) + eps_norm)
    ).astype(jnp.bfloat16)
    block_rows = lax.all_gather(normed, "tp", axis=0, tiled=True)
    gate_val = jnp.dot(block_rows, serve_shared_gate, preferred_element_type=jnp.float32)
    up_val = jnp.dot(block_rows, serve_shared_up, preferred_element_type=jnp.float32)
    shared_act = (jax.nn.silu(gate_val) * up_val).astype(jnp.bfloat16)
    shared_sum = lax.psum_scatter(
        jnp.dot(shared_act, serve_shared_down, preferred_element_type=jnp.float32).astype(
            jnp.bfloat16
        ),
        "tp",
        scatter_dimension=0,
        tiled=True,
    ).astype(jnp.float32)
    row_count = prompt.shape[0]
    top_count = expert_ids.shape[1]
    model_width = prompt.shape[1]
    expert_count = lax.axis_size("fs") * lax.axis_size("tp")
    capacity = row_count * top_count // expert_count + 1
    flat_ids = expert_ids.reshape(-1)
    onehot = (flat_ids[:, None] == jnp.arange(expert_count, dtype=jnp.int32)[None, :]).astype(
        jnp.int32
    )
    earlier = jnp.cumsum(onehot, axis=0) - onehot
    places = jnp.sum(earlier * onehot, axis=1)
    slot_ids = (flat_ids * capacity + places).reshape(row_count, top_count)
    slot_range = jnp.arange(expert_count * capacity, dtype=jnp.int32)
    dispatch = jnp.any(slot_range[:, None, None] == slot_ids[None, :, :], axis=-1).astype(
        jnp.bfloat16
    )
    outgoing = jnp.dot(dispatch, normed, preferred_element_type=jnp.float32).astype(jnp.bfloat16)
    outgoing = outgoing.reshape(expert_count, capacity, model_width)
    arrived = lax.all_to_all(outgoing, ("fs", "tp"), split_axis=0, concat_axis=0, tiled=True)
    source_count, slot_count, width_here = arrived.shape
    arrived_rows = arrived.reshape(source_count * slot_count, width_here)
    gate_val = jnp.dot(arrived_rows, serve_gate[0], preferred_element_type=jnp.float32)
    up_val = jnp.dot(arrived_rows, serve_up[0], preferred_element_type=jnp.float32)
    hidden = (jax.nn.silu(gate_val) * up_val).astype(jnp.bfloat16)
    result = jnp.dot(hidden, lowered[0], preferred_element_type=jnp.float32).astype(jnp.bfloat16)
    result = result.reshape(source_count, slot_count, width_here)
    returned = lax.all_to_all(result, ("fs", "tp"), split_axis=0, concat_axis=0, tiled=True)
    picked = returned.reshape(expert_count * capacity, model_width)[slot_ids]
    routed = jnp.sum(route_weight[:, :, None] * picked.astype(jnp.float32), axis=1)
    mixed_out = (routed + shared_sum).astype(jnp.bfloat16)
    return (
        serve_gate,
        serve_up,
        lowered,
        serve_shared_gate,
        serve_shared_up,
        serve_shared_down,
        mixed_out,
    )


def solution(mesh):
    placed = (
        P(("gr", "fs", "tp"), None),
        P(None, ("gr", "fs"), "tp"),
        P(None, ("gr", "fs"), "tp"),
        P(None, "tp", ("gr", "fs")),
        P(("gr", "fs"), "tp"),
        P(("gr", "fs"), "tp"),
        P("tp", ("gr", "fs")),
        P(("gr", "fs")),
        P(("gr", "fs", "tp"), None),
        P(("gr", "fs", "tp"), None),
    )
    n_gr, n_fs, n_tp = (mesh.shape[name] for name in ("gr", "fs", "tp"))

    def chosen(prompt, train_gate, *rest):
        rows, width = prompt.shape
        experts, cols, hid = train_gate.shape
        held = n_fs * n_tp * n_gr * CORES * 3 * hid * cols * 4 + 4 * n_fs * prompt.size * 2
        fits = n_gr == 2 and n_tp == 2 * CORES and n_fs % 2 == 0 and held < VMEM_PLAN
        even = experts == n_fs * n_tp and cols * n_gr * n_fs == width and rows == 128
        if fits and even and hid % (16 * n_fs) == 0 and cols % 128 == 0:
            return line_body(n_gr, n_fs, n_tp, prompt, train_gate, *rest)
        return body(prompt, train_gate, *rest)

    return jax.shard_map(
        chosen,
        mesh=mesh,
        in_specs=placed,
        out_specs=(
            P(("fs", "tp"), None, None),
            P(("fs", "tp"), None, None),
            P(("fs", "tp"), None, None),
            P(None, "tp"),
            P(None, "tp"),
            P("tp", None),
            P(("gr", "fs", "tp"), None),
        ),
        check_vma=False,
    )
```

```python
import functools

import jax
import jax.numpy as jnp
from jax import lax
from jax.experimental import pallas as pl
from jax.experimental.pallas import tpu as pltpu
from jax.sharding import PartitionSpec as P

eps_norm = 1e-06
MESH = pl.DeviceIdType.MESH
CORES = 2
PARTS = 4
VMEM_PLAN = 40 * 2**20
VMEM_LIMIT = 60 * 2**20


def line_kernel(
    n_gr, n_fs, n_tp, parts,
    p_hbm, gt_hbm, ut_hbm, dn_hbm, tsg_hbm, tsu_hbm, tsd_hbm, gain_hbm, ids_hbm, rw_hbm,
    gate_hbm, up_hbm, down_hbm, sg_hbm, su_hbm, sd_hbm, mixed_hbm,
    p_ref, gt_ref, ut_ref, dn_ref, sg_ref, su_ref, sd_ref, gain_ref, ids_ref, rw_ref,
    x_all, t_all, e_in, w_all, s_in, s_all, gate_out, up_out, acc, act, base, mixed_out,
    part, ru, rd,
    xr, tr, er, sr, sc, fr, ur, dr,
    zs, zd, xs, ys, xd, yd, fs_, ss, sx, sy, sd, us, ds_, loc, res_sem, in_sem,
):
    gr, z, tp = lax.axis_index("gr"), lax.axis_index("fs"), lax.axis_index("tp")
    y, c = tp // CORES, tp % CORES
    sides = n_tp // CORES
    x_peer, y_other, c_other = 1 - gr, 1 - y, 1 - c
    _, hid, cols = s_in.shape
    sub, width = x_all.shape[2], x_all.shape[3]
    rows = parts * sub
    full = n_gr * n_fs
    wide_hid = n_tp * hid

    def dev(g, f, t):
        return {"gr": g, "fs": f, "tp": t}

    to_x, to_y = dev(x_peer, z, tp), dev(gr, z, y_other * CORES + c)
    to_c = dev(gr, z, y * CORES + c_other)
    up, down = dev(gr, z + 1, tp), dev(gr, z - 1, tp)
    has_up, has_down = z < n_fs - 1, z > 0
    inner = has_up & has_down
    outer = jnp.logical_not(inner)

    def far(p):
        if p == n_fs - 1:
            return z
        fall, rise = n_fs - 1 - p, p
        fall = jnp.where(fall <= z, fall - 1, fall)
        rise = jnp.where(rise >= z, rise + 1, rise)
        return jnp.where(z < n_fs // 2, fall, rise)

    order = [far(n_fs - 1 - p) for p in range(n_fs)]

    def place(f, at):
        rise = jnp.where(f < at, f + 1, f)
        fall = jnp.where(f > at, n_fs - f, n_fs - 1 - f)
        return jnp.where(f == at, 0, jnp.where(at < n_fs // 2, rise, fall))

    first = pltpu.make_async_copy(gain_hbm, gain_ref, in_sem.at[0])
    first.start()
    heavy = []
    for p in range(n_fs):
        at = pl.ds(order[p] * n_tp, n_tp)
        heavy.append([
            pltpu.make_async_copy(src.at[at], dst.at[at], in_sem.at[1 + 3 * p + i])
            for i, (src, dst) in enumerate(((gt_hbm, gt_ref), (ut_hbm, ut_ref), (dn_hbm, dn_ref)))
        ])
    light = [
        pltpu.make_async_copy(src, dst, in_sem.at[1 + 3 * n_fs + i])
        for i, (src, dst) in enumerate((
            (tsg_hbm, sg_ref), (tsu_hbm, su_ref), (tsd_hbm, sd_ref), (p_hbm, p_ref),
            (ids_hbm, ids_ref), (rw_hbm, rw_ref),
        ))
    ]
    for one in sum(heavy, []) + light:
        one.start()

    barrier = pltpu.get_barrier_semaphore()

    def greet(where):
        pl.semaphore_signal(barrier, inc=1, device_id=where, device_id_type=MESH)

    for dz in range(n_fs):
        for dc in range(CORES):
            if dz or dc:
                greet(dev(gr, (z + dz) % n_fs, y * CORES + (c + dc) % CORES))
    greet(to_x)
    greet(to_y)

    first.wait()
    gain = gain_ref[...]

    def cast(p):
        for one in heavy[p]:
            one.wait()
        f = order[p]
        for t in range(n_tp):
            i = f * n_tp + t
            e_in[f, t % CORES, t // CORES, 0] = (gt_ref[i] * gain).astype(jnp.bfloat16)
            e_in[f, t % CORES, t // CORES, 1] = (ut_ref[i] * gain).astype(jnp.bfloat16)
            e_in[f, t % CORES, t // CORES, 2] = dn_ref[i].astype(jnp.bfloat16)

    cast(0)
    pl.semaphore_wait(barrier, n_fs * CORES + 1)

    def remote(src, dst, send, recv, where):
        return pltpu.make_async_remote_copy(
            src_ref=src, dst_ref=dst, send_sem=send, recv_sem=recv,
            device_id=where, device_id_type=MESH,
        )

    pending = []

    def when(cond, f):
        if cond is None:
            f()
        else:
            pl.when(cond)(f)

    def go(cond, copies, drain=True):
        if drain:
            pending.append((cond, copies))

        def start():
            for one in copies:
                one.start()

        when(cond, start)

    def drain(cond, ref, sem):
        pending.append((cond, [remote(ref, ref, sem, sc.at[0], to_c)]))

    def slab(g, f, t, core):
        at = pl.ds(pl.multiple_of(t * hid, hid), hid)
        return w_all.at[g * n_fs + f, core, :, :, at, :]

    def got(g, f, t):
        return er.at[(g * n_fs + f) * n_tp + t]

    def send_expert(p, i):
        f = order[p]
        core = c if i == 0 else c_other
        go(None, [remote(
            e_in.at[f, core], slab(gr, z, tp, core), zs.at[1 if p == 1 else 2],
            got(gr, z, tp), dev(gr, f, y * CORES + core),
        )], False)

    def wait_slab(g, f, t):
        remote(e_in.at[0, 0], slab(g, f, t, c), zs.at[0], got(g, f, t), to_x).wait_recv()

    def pass_slab(g, f, t, sem, where, src=None):
        place = slab(g, f, t, c)
        return remote(place if src is None else src, place, sem, got(g, f, t), where)

    def send_rows(cond, f, h, slot, way):
        to = z + 1 if way == 0 else z - 1
        here, there = place(f, z), place(f, to)
        where = dev(gr, to, tp)
        sem = zd.at[slot, 0]
        go(cond, [remote(x_all.at[here, h], x_all.at[there, h], sem, xr.at[f, h], where)], False)
        if h == 0:
            drain(cond, x_all.at[0], sem)
            go(cond, [remote(t_all.at[f], t_all.at[f], zd.at[slot, 1], tr.at[f], where)])

    def s_slice(t):
        return s_all.at[:, pl.ds(pl.multiple_of(t * hid, hid), hid), :]

    def s_slab(g, f, t):
        lanes = pl.ds(pl.multiple_of((g * n_fs + f) * cols, 128), cols)
        return s_all.at[:, pl.ds(pl.multiple_of(t * hid, hid), hid), lanes]

    def s_copy(src, g, f, sem, where, t=tp):
        src = s_slab(g, f, t) if src is None else src
        recv = sr.at[full] if where is to_y else sr.at[g * n_fs + f]
        return remote(src, s_slab(g, f, t), sem, recv, where)

    mine = e_in.at[z, c]
    go(None, [remote(
        e_in.at[z, c_other], slab(gr, z, tp, c_other), zs.at[0], got(gr, z, tp), to_c
    )])
    go(None, [pass_slab(gr, z, tp, xs.at[0], to_x, mine)], False)
    go(None, [pass_slab(gr, z, tp, ys.at[0], to_y, mine)], False)
    cast(1)
    for i in range(CORES):
        send_expert(1, i)
    for p in range(2, n_fs):
        cast(p)
    for i in range(CORES):
        for p in range(2, n_fs):
            send_expert(p, i)
    drain(None, w_all.at[0, 0, 0], zs.at[1])
    drain(None, w_all.at[0, 0], zs.at[2])
    drain(None, w_all.at[0], xs.at[0])
    drain(None, w_all.at[0], ys.at[0])
    drain(None, w_all.at[0, 0], xd.at[0])
    drain(None, w_all.at[0, 0], yd.at[0])
    drain(None, w_all.at[0 : full // 2], fs_.at[0])
    drain(None, w_all.at[0, 0, 0], sx.at[0])
    drain(None, s_slice(tp), sy.at[0])
    near_slab = pltpu.make_async_copy(mine, slab(gr, z, tp, c), loc.at[0])
    near_slab.start()

    for one in light:
        one.wait()
    s_in[0] = (sg_ref[...] * gain).astype(jnp.bfloat16)
    s_in[1] = (su_ref[...] * gain).astype(jnp.bfloat16)
    s_in[2] = sd_ref[...].astype(jnp.bfloat16)
    for h in range(parts):
        v = p_ref[h * sub : (h + 1) * sub, :].astype(jnp.float32)
        mean = jnp.mean(v * v, axis=-1, keepdims=True)
        x_all[0, h] = (v * lax.rsqrt(mean + eps_norm)).astype(jnp.bfloat16)
    shape = t_all.shape[1:]
    table = jnp.zeros(shape, jnp.float32)
    which = lax.broadcasted_iota(jnp.int32, shape, 0)
    for k in range(ids_ref.shape[0]):
        table = table + jnp.where(ids_ref[k : k + 1, :] == which, rw_ref[k : k + 1, :], 0.0)
    t_all[z] = table

    near_s = pltpu.make_async_copy(s_in, s_slab(gr, z, tp), loc.at[1])
    near_s.start()

    def send_own(cond):
        for h in range(parts):
            for way in (0, 1):
                there = has_up if way == 0 else has_down
                send_rows(there & cond, z, h, way, way)
        go(has_up & cond, [s_copy(s_in, gr, z, ss.at[0], up)])
        go(has_down & cond, [s_copy(s_in, gr, z, ss.at[1], down)])

    send_own(True)

    def own(p, i):
        f = order[p]
        core = c if i == 0 else c_other
        t = y * CORES + core
        wait_slab(gr, f, t)
        go(None, [pass_slab(gr, f, t, xs.at[0], to_x)], False)
        go(None, [pass_slab(gr, f, t, ys.at[0], to_y)], False)

    def result_copies(k):
        at = pl.ds(pl.multiple_of(k * cols, 128), cols)
        return [
            pltpu.make_async_copy(gate_out.at[at, :], gate_hbm.at[at, :], res_sem.at[0]),
            pltpu.make_async_copy(up_out.at[at, :], up_hbm.at[at, :], res_sem.at[1]),
            pltpu.make_async_copy(w_all.at[k, c, y, 2], down_hbm.at[:, at], res_sem.at[2]),
        ]

    half = wide_hid // sides

    def half_copy(k, core, part_of):
        at = pl.ds(pl.multiple_of(part_of * half, half), half)
        place_of = w_all.at[k, core, :, :, at, :]
        return remote(place_of, place_of, fs_.at[0], fr.at[k, part_of], to_c)

    def give(g, f, part_of):
        go(None, [half_copy(g * n_fs + f, c, part_of)], False)

    def turn(g, f):
        k = g * n_fs + f
        at = pl.ds(pl.multiple_of(k * cols, 128), cols)
        gate_out[at, :] = w_all[k, c, y, 0].T
        up_out[at, :] = w_all[k, c, y, 1].T
        for one in result_copies(k):
            one.start()

    def side(p, i):
        f = order[p]
        core = c if i == 0 else c_other
        wait_slab(x_peer, f, y * CORES + core)
        if (p + i) % 2 == 0:
            go(None, [pass_slab(x_peer, f, y * CORES + core, yd.at[0], to_y)], False)
        wait_slab(gr, f, y_other * CORES + core)
        if (p + i) % 2 == 1:
            go(None, [pass_slab(gr, f, y_other * CORES + core, xd.at[0], to_x)], False)
        if i == CORES - 1:
            give(x_peer, f, y)

    def column(p):
        if p == 0:
            near_slab.wait()
        give(gr, order[p], y)
        give(gr, order[p], y_other)
        turn(gr, order[p])

    def corner(p):
        f = order[p]
        for core in range(CORES):
            wait_slab(x_peer, f, y_other * CORES + core)
        give(x_peer, f, y_other)

    def corner_turn(p):
        turn(x_peer, order[p])

    def row_part(p, h, most=None):
        f = order[p]

        def arrive():
            remote(x_all.at[p, h], x_all.at[p, h], zd.at[0, 0], xr.at[f, h], to_x).wait_recv()
            if h == 0:
                remote(t_all.at[f], t_all.at[f], zd.at[0, 0], tr.at[f], to_x).wait_recv()

        when(most, arrive)
        if most is inner:
            send_rows((f < z) & inner, f, h, 1 + p, 0)
            send_rows((f > z) & inner, f, h, n_fs + p, 1)

    def wait_shared(g, f, t):
        s_copy(None, g, f, sx.at[0], to_x, t).wait_recv()

    def shared(p, most=True):
        f = order[p]
        src = None if p else s_in
        if p:
            when(None if most is True else most, functools.partial(wait_shared, gr, f, tp))
            go((f < z) & has_up & most, [s_copy(src, gr, f, ss.at[1 + p], up)])
            go((f > z) & has_down & most, [s_copy(src, gr, f, ss.at[n_fs + p], down)])
        most = None if most is True else most
        go(most, [s_copy(src, gr, f, sx.at[0], to_x)], False)
        go(most, [s_copy(src, gr, f, sy.at[0], to_y)], False)

    def shared_x(p):
        f = order[p]
        wait_shared(x_peer, f, tp)
        go(None, [s_copy(None, x_peer, f, sy.at[0], to_y)], False)

    def nt(a, b):
        return lax.dot_general(a, b, (((1,), (1,)), ((), ())), preferred_element_type=jnp.float32)

    def arrived(g, f):
        for side_of in range(sides):
            half_copy(g * n_fs + f, c_other, side_of).wait_recv()

    def add(k, lo, hi, first):
        at = pl.ds(pl.multiple_of(k * cols, 128), cols)
        lhs = x_all[lo:hi, :, :, at].reshape((hi - lo) * rows, cols)
        here = slice(lo * rows, hi * rows)
        for s in range(n_tp):
            w = w_all[k, s // sides, s % sides, 0:2].reshape(2 * wide_hid, cols)
            val = nt(lhs, w)
            acc[s, here] = val if first else acc[s, here] + val

    def step(g, f, lo, hi, first=False):
        add(g * n_fs + f, lo, hi, first)

    def late(lo, hi):
        some = (hi - lo) * sub
        lhs = x_all[n_fs - 1, lo:hi].reshape(some, width)
        here = (n_fs - 1) * rows + lo * sub

        def one(s, carry):
            total = None
            for k in range(full):
                w = w_all[k, s // sides, s % sides, 0:2].reshape(2 * wide_hid, cols)
                val = nt(lhs[:, k * cols : (k + 1) * cols], w)
                total = val if total is None else total + val
            acc[s, here : here + some] = total
            return carry

        lax.fori_loop(0, n_tp, one, 0)

    def s_whole(t, i):
        return remote(s_slice(t), s_slice(t), sd.at[i], sc.at[t], to_c)

    s_results = [
        pltpu.make_async_copy(s_slice(tp).at[i], dst, res_sem.at[3 + i])
        for i, dst in enumerate((sg_hbm, su_hbm, sd_hbm))
    ]
    t_y = y_other * CORES + c

    def shared_give():
        near_s.wait()
        go(None, [s_whole(tp, 0)])
        for one in s_results:
            one.start()
        remote(s_slice(t_y), s_slice(t_y), sy.at[0], sr.at[full], to_y).wait_recv()
        go(None, [s_whole(t_y, 1)])

    def shared_act():
        for side in range(sides):
            s_whole(side * CORES + c_other, 0).wait_recv()
        lhs = x_all[0].reshape(rows, width)
        both = nt(lhs, s_all[0:2].reshape(2 * wide_hid, width))
        act[0] = (jax.nn.silu(both[:, :wide_hid]) * both[:, wide_hid:]).astype(jnp.bfloat16)

        def columns(k, inner):
            at = pl.ds(pl.multiple_of(k * cols, 128), cols)
            val = jnp.dot(act[0], s_all[2, :, at], preferred_element_type=jnp.float32)
            base[:, at] = val
            return inner

        lax.fori_loop(0, full, columns, 0)

    stages = []

    def then(f, *args):
        stages.append((f, args))

    def only(cond, f, *args):
        @functools.wraps(f)
        def run(*given):
            pl.when(cond)(lambda: f(*given))

        stages.append((run, args))

    def wide(v):
        return v.astype(jnp.float32)

    def u_copy(t, h):
        return remote(part.at[t, h], ru.at[t, h], us.at[t], ur.at[t, h], up)

    def d_copy(t, h):
        return remote(part.at[t, h], rd.at[t, h], ds_.at[t], dr.at[t, h], down)

    def when_way(t, ahead, behind):
        pl.when(t > z)(ahead)
        pl.when(t < z)(behind)

    def block(p, lo=0, hi=parts):
        t = order[p]
        some, skip = (hi - lo) * sub, lo * sub
        here = slice(p * rows + skip, p * rows + skip + some)

        for s in range(n_tp):
            e = z * n_tp + (s % sides) * CORES + s // sides
            scale = jnp.broadcast_to(t_all[t, pl.ds(e, 1), :], (rows, rows)).T
            scale = scale[skip : skip + some, :1]
            val = acc[s, here, :]
            val = jax.nn.silu(val[:, :wide_hid]) * val[:, wide_hid:] * scale
            act[s, 0:some] = val.astype(jnp.bfloat16)

        group = 4

        def columns(j, carry):
            for i in range(group):
                k = j * group + i
                at = pl.ds(pl.multiple_of(k * cols, 128), cols)
                total = None
                for s in range(n_tp):
                    val = jnp.dot(
                        act[s, 0:some], w_all[k, s // sides, s % sides, 2],
                        preferred_element_type=jnp.float32,
                    )
                    total = val if total is None else total + val
                total = total.astype(jnp.bfloat16)
                part[t, lo:hi, :, at] = total.reshape(hi - lo, sub, cols)
            return carry

        lax.fori_loop(0, full // group, columns, 0)
        if p:
            for g in range(lo, hi):
                pl.when((t > z) & jnp.logical_not(has_down))(lambda g=g: u_copy(t, g).start())
                pl.when((t < z) & jnp.logical_not(has_up))(lambda g=g: d_copy(t, g).start())

    def chain(p, lo=0, hi=parts):
        t = order[p]
        for h in range(lo, hi):
            for copy, arrived, cond in (
                (u_copy, ru, (t > z) & has_down), (d_copy, rd, (t < z) & has_up)
            ):

                @pl.when(cond)
                def _(h=h, copy=copy, arrived=arrived):
                    with jax.named_scope("chain"):
                        copy(t, h).wait_recv()
                    part[t, h] = (wide(part[t, h]) + wide(arrived[t, h])).astype(jnp.bfloat16)
                    copy(t, h).start()

    def mixed_copy(h):
        return pltpu.make_async_copy(mixed_out.at[h], mixed_hbm.at[h], loc.at[2 + h])

    def finish(h):
        mine_h = slice(h * sub, (h + 1) * sub)

        def total(*arrived):
            val = wide(part[z, h]) + base[mine_h, :]
            for one in arrived:
                val = val + wide(one)
            mixed_out[h] = val.astype(jnp.bfloat16)

        @pl.when(has_down & has_up)
        def _():
            u_copy(z, h).wait_recv()
            d_copy(z, h).wait_recv()
            total(ru[z, h], rd[z, h])

        @pl.when(jnp.logical_not(has_up))
        def _():
            u_copy(z, h).wait_recv()
            total(ru[z, h])

        @pl.when(jnp.logical_not(has_down))
        def _():
            d_copy(z, h).wait_recv()
            total(rd[z, h])

        mixed_copy(h).start()

    last, half_way = n_fs - 1, parts // 2
    then(own, 0, 1)
    then(own, 1, 0)
    then(own, 1, 1)
    then(side, 0, 0)
    then(side, 0, 1)
    then(column, 0)
    for p in range(2, n_fs):
        then(own, p, 0)
    then(side, 1, 0)
    then(side, 1, 1)
    then(column, 1)
    for p in range(2, n_fs):
        then(own, p, 1)
    for p in range(2, n_fs):
        then(side, p, 0)
    for h in range(half_way):
        then(row_part, 1, h, inner)
    then(row_part, 2, 0, inner)
    for h in range(half_way, parts):
        then(row_part, 1, h, inner)
    then(side, 2, 1)
    for h in range(1, parts - 1):
        then(row_part, 2, h, inner)
    then(side, last, 1)
    then(row_part, 2, parts - 1, inner)
    then(column, 2)
    then(column, last)
    then(corner, 0)
    then(corner, 1)
    for h in range(parts):
        then(row_part, 1, h, outer)
    then(shared, 0)
    then(shared, 1, outer)
    then(corner_turn, 0)
    then(corner_turn, 1)
    for p in range(n_fs):
        then(arrived, gr, order[p])
        then(step, gr, order[p], 0, 2, p == 0)
    for p in range(2):
        then(arrived, x_peer, order[p])
        then(step, x_peer, order[p], 0, 2)
    for h in range(half_way):
        then(row_part, last, h, inner)
    for h in range(parts):
        then(row_part, 2, h, outer)
    then(step, gr, order[0], 2, 3, True)
    then(step, gr, order[1], 2, 3)
    then(corner, 2)
    for h in range(half_way, parts - 1):
        then(row_part, last, h, inner)
    for p in range(2, n_fs):
        then(step, gr, order[p], 2, 3)
    then(row_part, last, parts - 1, inner)
    then(shared, 1, inner)
    then(shared, 2, inner)
    then(corner, last)
    for p in range(2):
        then(step, x_peer, order[p], 2, 3)
    for p in range(2, n_fs):
        then(arrived, x_peer, order[p])
        then(step, x_peer, order[p], 0, 3)
    then(block, last - 1)
    only(inner, late, 0, parts)
    only(inner, block, last, 0, parts)
    for lo, hi in ((0, half_way), (half_way, parts)):
        for h in range(lo, hi):
            then(row_part, last, h, outer)
        only(outer, late, lo, hi)
        only(outer, block, last, lo, hi)
    then(shared, last, inner)
    then(chain, last - 1, 0, half_way)
    then(block, 1)
    then(shared, 2, outer)
    then(block, 0)
    then(chain, last - 1, half_way, parts)
    then(corner_turn, 2)
    then(corner_turn, last)
    then(shared, last, outer)
    then(shared_x, 0)
    then(shared_x, 1)
    then(chain, last, 0, half_way)
    then(shared_x, 2)
    then(shared_x, last)
    then(chain, last, half_way, parts)
    for p in range(1, last - 1):
        then(chain, p, 0, half_way)
    then(shared_give)
    for p in range(1, last - 1):
        then(chain, p, half_way, parts)
    then(shared_act)
    for h in range(parts):
        then(finish, h)

    for f, args in stages:
        with jax.named_scope(f.__name__ + "_".join(str(a) for a in args if type(a) is int)):
            f(*args)

    with jax.named_scope("drain"):
        for h in range(parts):
            mixed_copy(h).wait()
        for one in s_results:
            one.wait()
        for i, (src, dst) in enumerate((
            (gate_out, gate_hbm), (up_out, up_hbm), (gate_out, gate_hbm),
        )):
            pltpu.make_async_copy(src, dst, res_sem.at[i]).wait()
        for cond, copies in pending:
            when(cond, lambda copies=copies: [one.wait_send() for one in copies] and None)
        for t in range(n_fs):
            whole = part.at[t]
            pl.when(t > z)(lambda: remote(whole, whole, us.at[t], ur.at[t, 0], up).wait_send())
            pl.when(t < z)(lambda: remote(whole, whole, ds_.at[t], dr.at[t, 0], down).wait_send())


def copy_kernel(count, *refs):
    ins, outs, bufs, sems = refs[:count], refs[count : 2 * count], refs[2 * count : -1], refs[-1]
    loads = [pltpu.make_async_copy(ins[i], bufs[i], sems.at[0, i]) for i in range(count)]
    stores = [pltpu.make_async_copy(bufs[i], outs[i], sems.at[1, i]) for i in range(count)]
    for one in loads:
        one.start()
    for one, then in zip(loads, stores):
        one.wait()
        then.start()
    for one in stores:
        one.wait()


def copied(arrays):
    count = len(arrays)
    return pl.pallas_call(
        functools.partial(copy_kernel, count),
        out_shape=tuple(jax.ShapeDtypeStruct(a.shape, a.dtype) for a in arrays),
        in_specs=[pl.BlockSpec(memory_space=pl.ANY)] * count,
        out_specs=(pl.BlockSpec(memory_space=pl.ANY),) * count,
        scratch_shapes=[pltpu.VMEM(a.shape, a.dtype) for a in arrays]
        + [pltpu.SemaphoreType.DMA((2, count))],
        compiler_params=pltpu.CompilerParams(vmem_limit_bytes=VMEM_LIMIT),
    )(*arrays)


def line_body(
    n_gr, n_fs, n_tp,
    prompt, train_gate, train_up, train_down, train_shared_gate, train_shared_up,
    train_shared_down, norm_gain, expert_ids, route_weight,
):
    experts, cols, hid = train_gate.shape
    rows, width = prompt.shape
    full, parts, sides = n_gr * n_fs, PARTS, n_tp // CORES
    sub, wide_hid = rows // parts, n_tp * hid
    bf16 = jnp.bfloat16
    f32 = jnp.float32
    hbm = pl.BlockSpec(memory_space=pl.ANY)
    dma = pltpu.SemaphoreType.DMA
    shape = jax.ShapeDtypeStruct
    outs = pl.pallas_call(
        functools.partial(line_kernel, n_gr, n_fs, n_tp, parts),
        out_shape=(
            shape((width, wide_hid), bf16),
            shape((width, wide_hid), bf16),
            shape((wide_hid, width), bf16),
            shape((hid, width), bf16),
            shape((hid, width), bf16),
            shape((hid, width), bf16),
            shape((parts, sub, width), bf16),
        ),
        in_specs=[hbm] * 10,
        out_specs=(hbm,) * 7,
        scratch_shapes=[
            pltpu.VMEM((rows, width), bf16),
            pltpu.VMEM((experts, hid, cols), f32),
            pltpu.VMEM((experts, hid, cols), f32),
            pltpu.VMEM((experts, hid, cols), f32),
            pltpu.VMEM((hid, cols), f32),
            pltpu.VMEM((hid, cols), f32),
            pltpu.VMEM((hid, cols), f32),
            pltpu.VMEM((1, cols), f32),
            pltpu.VMEM((expert_ids.shape[1], rows), jnp.int32),
            pltpu.VMEM((expert_ids.shape[1], rows), f32),
            pltpu.VMEM((n_fs, parts, sub, width), bf16),
            pltpu.VMEM((n_fs, experts, rows), f32),
            pltpu.VMEM((n_fs, CORES, sides, 3, hid, cols), bf16),
            pltpu.VMEM((full, CORES, sides, 3, wide_hid, cols), bf16),
            pltpu.VMEM((3, hid, cols), bf16),
            pltpu.VMEM((3, wide_hid, width), bf16),
            pltpu.VMEM((width, wide_hid), bf16),
            pltpu.VMEM((width, wide_hid), bf16),
            pltpu.VMEM((n_tp, n_fs * rows, 2 * wide_hid), f32),
            pltpu.VMEM((n_tp, rows, wide_hid), bf16),
            pltpu.VMEM((rows, width), f32),
            pltpu.VMEM((parts, sub, width), bf16),
            pltpu.VMEM((n_fs, parts, sub, width), bf16),
            pltpu.VMEM((n_fs, parts, sub, width), bf16),
            pltpu.VMEM((n_fs, parts, sub, width), bf16),
            dma((n_fs, parts)), dma((n_fs,)), dma((full * n_tp,)), dma((full + 1,)),
            dma((n_tp,)), dma((full, sides)), dma((n_fs, parts)), dma((n_fs, parts)),
            dma((3,)), dma((2 * n_fs, 2)), dma((1,)), dma((1,)), dma((1,)), dma((1,)),
            dma((1,)), dma((2 * n_fs,)), dma((1,)), dma((1,)), dma((2,)),
            dma((n_fs,)), dma((n_fs,)),
            dma((2 + parts,)), dma((6,)), dma((7 + 3 * n_fs,)),
        ],
        compiler_params=pltpu.CompilerParams(
            collective_id=0, has_side_effects=True, vmem_limit_bytes=VMEM_LIMIT
        ),
    )(
        prompt, train_gate.transpose(0, 2, 1), train_up.transpose(0, 2, 1), train_down,
        train_shared_gate.T, train_shared_up.T, train_shared_down, norm_gain[None, :],
        expert_ids.T, route_weight.T,
    )
    serve_gate, serve_up, serve_down, s_gate, s_up, s_down, mixed_out = copied(outs)
    return (
        serve_gate[None], serve_up[None], serve_down[None],
        s_gate.T, s_up.T, s_down, mixed_out.reshape(rows, width),
    )


def regroup(stacked, lowered):
    stacked = lax.all_to_all(
        lax.all_to_all(stacked, "fs", split_axis=0, concat_axis=2, tiled=True),
        "tp",
        split_axis=0,
        concat_axis=3,
        tiled=True,
    )
    lowered = lax.all_to_all(
        lax.all_to_all(lowered, "fs", split_axis=0, concat_axis=2, tiled=True),
        "tp",
        split_axis=0,
        concat_axis=1,
        tiled=True,
    )
    return (stacked, lowered)


def body(
    prompt,
    train_gate,
    train_up,
    train_down,
    train_shared_gate,
    train_shared_up,
    train_shared_down,
    norm_gain,
    expert_ids,
    route_weight,
):
    gain_col = norm_gain[:, None]
    stacked = jnp.stack((train_gate * gain_col[None], train_up * gain_col[None]), axis=1).astype(
        jnp.bfloat16
    )
    lowered = train_down.astype(jnp.bfloat16)
    stacked, lowered = regroup(stacked, lowered)
    stacked, lowered = (
        lax.all_gather(stacked, "gr", axis=2, tiled=True),
        lax.all_gather(lowered, "gr", axis=2, tiled=True),
    )
    serve_gate = stacked[:, 0]
    serve_up = stacked[:, 1]
    serve_shared_gate, serve_shared_up, serve_shared_down = (
        lax.all_gather(
            (train_shared_gate * gain_col).astype(jnp.bfloat16), ("gr", "fs"), axis=0, tiled=True
        ),
        lax.all_gather(
            (train_shared_up * gain_col).astype(jnp.bfloat16), ("gr", "fs"), axis=0, tiled=True
        ),
        lax.all_gather(train_shared_down.astype(jnp.bfloat16), ("gr", "fs"), axis=1, tiled=True),
    )
    widened = prompt.astype(jnp.float32)
    normed = (
        widened * lax.rsqrt(jnp.mean(widened * widened, axis=-1, keepdims=True) + eps_norm)
    ).astype(jnp.bfloat16)
    block_rows = lax.all_gather(normed, "tp", axis=0, tiled=True)
    gate_val = jnp.dot(block_rows, serve_shared_gate, preferred_element_type=jnp.float32)
    up_val = jnp.dot(block_rows, serve_shared_up, preferred_element_type=jnp.float32)
    shared_act = (jax.nn.silu(gate_val) * up_val).astype(jnp.bfloat16)
    shared_sum = lax.psum_scatter(
        jnp.dot(shared_act, serve_shared_down, preferred_element_type=jnp.float32).astype(
            jnp.bfloat16
        ),
        "tp",
        scatter_dimension=0,
        tiled=True,
    ).astype(jnp.float32)
    row_count = prompt.shape[0]
    top_count = expert_ids.shape[1]
    model_width = prompt.shape[1]
    expert_count = lax.axis_size("fs") * lax.axis_size("tp")
    capacity = row_count * top_count // expert_count + 1
    flat_ids = expert_ids.reshape(-1)
    onehot = (flat_ids[:, None] == jnp.arange(expert_count, dtype=jnp.int32)[None, :]).astype(
        jnp.int32
    )
    earlier = jnp.cumsum(onehot, axis=0) - onehot
    places = jnp.sum(earlier * onehot, axis=1)
    slot_ids = (flat_ids * capacity + places).reshape(row_count, top_count)
    slot_range = jnp.arange(expert_count * capacity, dtype=jnp.int32)
    dispatch = jnp.any(slot_range[:, None, None] == slot_ids[None, :, :], axis=-1).astype(
        jnp.bfloat16
    )
    outgoing = jnp.dot(dispatch, normed, preferred_element_type=jnp.float32).astype(jnp.bfloat16)
    outgoing = outgoing.reshape(expert_count, capacity, model_width)
    arrived = lax.all_to_all(outgoing, ("fs", "tp"), split_axis=0, concat_axis=0, tiled=True)
    source_count, slot_count, width_here = arrived.shape
    arrived_rows = arrived.reshape(source_count * slot_count, width_here)
    gate_val = jnp.dot(arrived_rows, serve_gate[0], preferred_element_type=jnp.float32)
    up_val = jnp.dot(arrived_rows, serve_up[0], preferred_element_type=jnp.float32)
    hidden = (jax.nn.silu(gate_val) * up_val).astype(jnp.bfloat16)
    result = jnp.dot(hidden, lowered[0], preferred_element_type=jnp.float32).astype(jnp.bfloat16)
    result = result.reshape(source_count, slot_count, width_here)
    returned = lax.all_to_all(result, ("fs", "tp"), split_axis=0, concat_axis=0, tiled=True)
    picked = returned.reshape(expert_count * capacity, model_width)[slot_ids]
    routed = jnp.sum(route_weight[:, :, None] * picked.astype(jnp.float32), axis=1)
    mixed_out = (routed + shared_sum).astype(jnp.bfloat16)
    return (
        serve_gate,
        serve_up,
        lowered,
        serve_shared_gate,
        serve_shared_up,
        serve_shared_down,
        mixed_out,
    )


def solution(mesh):
    placed = (
        P(("gr", "fs", "tp"), None),
        P(None, ("gr", "fs"), "tp"),
        P(None, ("gr", "fs"), "tp"),
        P(None, "tp", ("gr", "fs")),
        P(("gr", "fs"), "tp"),
        P(("gr", "fs"), "tp"),
        P("tp", ("gr", "fs")),
        P(("gr", "fs")),
        P(("gr", "fs", "tp"), None),
        P(("gr", "fs", "tp"), None),
    )
    n_gr, n_fs, n_tp = (mesh.shape[name] for name in ("gr", "fs", "tp"))

    def chosen(prompt, train_gate, *rest):
        rows, width = prompt.shape
        experts, cols, hid = train_gate.shape
        held = n_fs * n_tp * n_gr * CORES * 3 * hid * cols * 4 + 4 * n_fs * prompt.size * 2
        fits = n_gr == 2 and n_tp == 2 * CORES and n_fs % 2 == 0 and held < VMEM_PLAN
        even = experts == n_fs * n_tp and cols * n_gr * n_fs == width and rows == 128
        if fits and even and hid % (16 * n_fs) == 0 and cols % 128 == 0:
            return line_body(n_gr, n_fs, n_tp, prompt, train_gate, *rest)
        return body(prompt, train_gate, *rest)

    return jax.shard_map(
        chosen,
        mesh=mesh,
        in_specs=placed,
        out_specs=(
            P(("fs", "tp"), None, None),
            P(("fs", "tp"), None, None),
            P(("fs", "tp"), None, None),
            P(None, "tp"),
            P(None, "tp"),
            P("tp", None),
            P(("gr", "fs", "tp"), None),
        ),
        check_vma=False,
    )
```

```python
import functools

import jax
import jax.numpy as jnp
from jax import lax
from jax.experimental import pallas as pl
from jax.experimental.pallas import tpu as pltpu
from jax.sharding import PartitionSpec as P

eps_norm = 1e-06
MESH = pl.DeviceIdType.MESH
CORES = 2
PARTS = 4
VMEM_PLAN = 40 * 2**20
VMEM_LIMIT = 119 * 2**19
COPY_LIMIT = 4 * 2**20


def line_kernel(
    n_gr, n_fs, n_tp, parts,
    p_hbm, gt_hbm, ut_hbm, dn_hbm, tsg_hbm, tsu_hbm, tsd_hbm, gain_hbm, ids_hbm, rw_hbm,
    gate_hbm, up_hbm, down_hbm, sg_hbm, su_hbm, sd_hbm, mixed_hbm,
    p_ref, gt_ref, ut_ref, dn_ref, sg_ref, su_ref, sd_ref, gain_ref, ids_ref, rw_ref,
    x_all, t_all, e_in, w_all, s_in, s_all, gate_out, up_out, acc, act, base, mixed_out,
    part, ru, rd,
    xr, tr, er, sr, sc, fr, cr,
    zs, zd, xs, ys, xd, yd, fs_, ss, sx, sy, sd, us, loc, res_sem, in_sem,
):
    gr, z, tp = lax.axis_index("gr"), lax.axis_index("fs"), lax.axis_index("tp")
    y, c = tp // CORES, tp % CORES
    sides = n_tp // CORES
    x_peer, y_other, c_other = 1 - gr, 1 - y, 1 - c
    _, hid, cols = s_in.shape
    sub, width = x_all.shape[2], x_all.shape[3]
    rows = parts * sub
    full = n_gr * n_fs
    wide_hid = n_tp * hid

    def dev(g, f, t):
        return {"gr": g, "fs": f, "tp": t}

    to_x, to_y = dev(x_peer, z, tp), dev(gr, z, y_other * CORES + c)
    to_c = dev(gr, z, y * CORES + c_other)
    up, down = dev(gr, z + 1, tp), dev(gr, z - 1, tp)
    has_up, has_down = z < n_fs - 1, z > 0
    inner = has_up & has_down
    outer = jnp.logical_not(inner)

    def far(p):
        if p == n_fs - 1:
            return z
        fall, rise = n_fs - 1 - p, p
        fall = jnp.where(fall <= z, fall - 1, fall)
        rise = jnp.where(rise >= z, rise + 1, rise)
        return jnp.where(z < n_fs // 2, fall, rise)

    order = [far(n_fs - 1 - p) for p in range(n_fs)]

    def place(f, at):
        rise = jnp.where(f < at, f + 1, f)
        fall = jnp.where(f > at, n_fs - f, n_fs - 1 - f)
        return jnp.where(f == at, 0, jnp.where(at < n_fs // 2, rise, fall))

    first = pltpu.make_async_copy(gain_hbm, gain_ref, in_sem.at[0])
    first.start()
    heavy = []
    for p in range(n_fs):
        at = pl.ds(order[p] * n_tp, n_tp)
        heavy.append([
            pltpu.make_async_copy(src.at[at], dst.at[at], in_sem.at[1 + p])
            for src, dst in ((gt_hbm, gt_ref), (ut_hbm, ut_ref), (dn_hbm, dn_ref))
        ])
    light = [
        pltpu.make_async_copy(src, dst, in_sem.at[1 + n_fs + i])
        for i, (src, dst) in enumerate((
            (tsg_hbm, sg_ref), (tsu_hbm, su_ref), (tsd_hbm, sd_ref), (p_hbm, p_ref),
            (ids_hbm, ids_ref), (rw_hbm, rw_ref),
        ))
    ]
    for one in sum(heavy, []) + light:
        one.start()

    barrier = pltpu.get_barrier_semaphore()

    def greet(where):
        pl.semaphore_signal(barrier, inc=1, device_id=where, device_id_type=MESH)

    for dz in range(n_fs):
        for dc in range(CORES):
            if dz or dc:
                greet(dev(gr, (z + dz) % n_fs, y * CORES + (c + dc) % CORES))
    greet(to_x)
    greet(to_y)

    first.wait()
    gain = gain_ref[...]

    def cast(p):
        all_of = pl.ds(0, 3 * n_tp)
        pltpu.make_async_copy(gt_hbm.at[all_of], gt_ref.at[all_of], in_sem.at[1 + p]).wait()
        f = order[p]
        for t in range(n_tp):
            i = f * n_tp + t
            e_in[f, t % CORES, t // CORES, 0] = (gt_ref[i] * gain).astype(jnp.bfloat16)
            e_in[f, t % CORES, t // CORES, 1] = (ut_ref[i] * gain).astype(jnp.bfloat16)
            e_in[f, t % CORES, t // CORES, 2] = dn_ref[i].astype(jnp.bfloat16)

    with jax.named_scope("cast0"):
        cast(0)
    with jax.named_scope("greeted"):
        pl.semaphore_wait(barrier, n_fs * CORES + 1)

    def remote(src, dst, send, recv, where):
        return pltpu.make_async_remote_copy(
            src_ref=src, dst_ref=dst, send_sem=send, recv_sem=recv,
            device_id=where, device_id_type=MESH,
        )

    pending = []

    def when(cond, f):
        if cond is None:
            f()
        else:
            pl.when(cond)(f)

    def go(cond, copies, drain=True):
        if drain:
            pending.append((cond, copies))

        def start():
            for one in copies:
                one.start()

        when(cond, start)

    def drain(cond, ref, sem):
        pending.append((cond, [remote(ref, ref, sem, sc.at[0], to_c)]))

    def slab(g, f, t, core):
        at = pl.ds(pl.multiple_of(t * hid, hid), hid)
        return w_all.at[g * n_fs + f, core, :, :, at, :]

    def got(g, f, t):
        return er.at[(g * n_fs + f) * n_tp + t]

    def send_expert(p, i):
        f = order[p]
        core = c if i == 0 else c_other
        go(None, [remote(
            e_in.at[f, core], slab(gr, z, tp, core), zs.at[1 if p == 1 else 2],
            got(gr, z, tp), dev(gr, f, y * CORES + core),
        )], False)

    def wait_slab(g, f, t):
        remote(e_in.at[0, 0], slab(g, f, t, c), zs.at[0], got(g, f, t), to_x).wait_recv()

    def pass_slab(g, f, t, sem, where, src=None):
        place = slab(g, f, t, c)
        return remote(place if src is None else src, place, sem, got(g, f, t), where)

    def send_rows(cond, f, h, slot, way):
        to = z + 1 if way == 0 else z - 1
        here, there = place(f, z), place(f, to)
        where = dev(gr, to, tp)
        sem = zd.at[slot, 0]
        go(cond, [remote(x_all.at[here, h], x_all.at[there, h], sem, xr.at[f, h], where)], False)
        if h == 0:
            drain(cond, x_all.at[0], sem)
            go(cond, [remote(t_all.at[f], t_all.at[f], zd.at[slot, 1], tr.at[f], where)])

    def s_slice(t):
        return s_all.at[:, pl.ds(pl.multiple_of(t * hid, hid), hid), :]

    def s_slab(g, f, t):
        lanes = pl.ds(pl.multiple_of((g * n_fs + f) * cols, 128), cols)
        return s_all.at[:, pl.ds(pl.multiple_of(t * hid, hid), hid), lanes]

    def s_copy(src, g, f, sem, where, t=tp):
        src = s_slab(g, f, t) if src is None else src
        recv = sr.at[full] if where is to_y else sr.at[g * n_fs + f]
        return remote(src, s_slab(g, f, t), sem, recv, where)

    mine = e_in.at[z, c]
    go(None, [remote(
        e_in.at[z, c_other], slab(gr, z, tp, c_other), zs.at[0], got(gr, z, tp), to_c
    )])
    go(None, [pass_slab(gr, z, tp, xs.at[0], to_x, mine)], False)
    go(None, [pass_slab(gr, z, tp, ys.at[0], to_y, mine)], False)
    cast(1)
    for i in range(CORES):
        send_expert(1, i)
    for p in range(2, n_fs):
        cast(p)
    for i in range(CORES):
        for p in range(2, n_fs):
            send_expert(p, i)
    drain(None, w_all.at[0, 0, 0], zs.at[1])
    drain(None, w_all.at[0, 0], zs.at[2])
    drain(None, w_all.at[0], xs.at[0])
    drain(None, w_all.at[0], ys.at[0])
    drain(None, w_all.at[0, 0], xd.at[0])
    drain(None, w_all.at[0, 0], yd.at[0])
    drain(None, w_all.at[0 : full // 2], fs_.at[0])
    drain(None, w_all.at[0, 0, 0], sx.at[0])
    drain(None, s_slice(tp), sy.at[0])
    near_slab = pltpu.make_async_copy(mine, slab(gr, z, tp, c), loc.at[0])
    near_slab.start()

    for one in light:
        one.wait()
    s_in[0] = (sg_ref[...] * gain).astype(jnp.bfloat16)
    s_in[1] = (su_ref[...] * gain).astype(jnp.bfloat16)
    s_in[2] = sd_ref[...].astype(jnp.bfloat16)
    for h in range(parts):
        v = p_ref[h * sub : (h + 1) * sub, :].astype(jnp.float32)
        mean = jnp.mean(v * v, axis=-1, keepdims=True)
        x_all[0, h] = (v * lax.rsqrt(mean + eps_norm)).astype(jnp.bfloat16)
    shape = t_all.shape[1:]
    table = jnp.zeros(shape, jnp.float32)
    which = lax.broadcasted_iota(jnp.int32, shape, 0)
    for k in range(ids_ref.shape[0]):
        table = table + jnp.where(ids_ref[k : k + 1, :] == which, rw_ref[k : k + 1, :], 0.0)
    t_all[z] = table

    near_s = pltpu.make_async_copy(s_in, s_slab(gr, z, tp), loc.at[1])
    near_s.start()

    def send_own(cond):
        for h in range(parts):
            for way in (0, 1):
                there = has_up if way == 0 else has_down
                send_rows(there & cond, z, h, way, way)
        go(has_up & cond, [s_copy(s_in, gr, z, ss.at[0], up)])
        go(has_down & cond, [s_copy(s_in, gr, z, ss.at[1], down)])

    send_own(True)

    def own(p, i):
        f = order[p]
        core = c if i == 0 else c_other
        t = y * CORES + core
        wait_slab(gr, f, t)
        go(None, [pass_slab(gr, f, t, xs.at[0], to_x)], False)
        go(None, [pass_slab(gr, f, t, ys.at[0], to_y)], False)

    def result_copies(k):
        at = pl.ds(pl.multiple_of(k * cols, 128), cols)
        return [
            pltpu.make_async_copy(gate_out.at[at, :], gate_hbm.at[at, :], res_sem.at[0]),
            pltpu.make_async_copy(up_out.at[at, :], up_hbm.at[at, :], res_sem.at[1]),
            pltpu.make_async_copy(w_all.at[k, c, y, 2], down_hbm.at[:, at], res_sem.at[2]),
        ]

    half = wide_hid // sides

    def half_copy(k, core, part_of):
        at = pl.ds(pl.multiple_of(part_of * half, half), half)
        place_of = w_all.at[k, core, :, :, at, :]
        return remote(place_of, place_of, fs_.at[0], fr.at[k], to_c)

    def give(g, f, part_of):
        go(None, [half_copy(g * n_fs + f, c, part_of)], False)

    def turn(g, f):
        k = g * n_fs + f
        at = pl.ds(pl.multiple_of(k * cols, 128), cols)
        gate_out[at, :] = w_all[k, c, y, 0].T
        up_out[at, :] = w_all[k, c, y, 1].T
        for one in result_copies(k):
            one.start()

    def side(p, i):
        f = order[p]
        core = c if i == 0 else c_other
        wait_slab(x_peer, f, y * CORES + core)
        if (p + i) % 2 == 0:
            go(None, [pass_slab(x_peer, f, y * CORES + core, yd.at[0], to_y)], False)
        wait_slab(gr, f, y_other * CORES + core)
        if (p + i) % 2 == 1:
            go(None, [pass_slab(gr, f, y_other * CORES + core, xd.at[0], to_x)], False)
        if i == CORES - 1:
            give(x_peer, f, y)

    def column(p):
        if p == 0:
            near_slab.wait()
        give(gr, order[p], y)
        give(gr, order[p], y_other)
        turn(gr, order[p])

    def corner(p):
        f = order[p]
        for core in range(CORES):
            wait_slab(x_peer, f, y_other * CORES + core)
        give(x_peer, f, y_other)

    def corner_turn(p):
        turn(x_peer, order[p])

    def row_part(p, h, most=None):
        f = order[p]

        def arrive():
            remote(x_all.at[p, h], x_all.at[p, h], zd.at[0, 0], xr.at[f, h], to_x).wait_recv()
            if h == 0:
                remote(t_all.at[f], t_all.at[f], zd.at[0, 0], tr.at[f], to_x).wait_recv()

        when(most, arrive)
        if most is inner:
            send_rows((f < z) & inner, f, h, 1 + p, 0)
            send_rows((f > z) & inner, f, h, 1 + p, 1)

    def wait_shared(g, f, t):
        s_copy(None, g, f, sx.at[0], to_x, t).wait_recv()

    def shared(p, most=True):
        f = order[p]
        src = None if p else s_in
        if p:
            when(None if most is True else most, functools.partial(wait_shared, gr, f, tp))
            go((f < z) & has_up & most, [s_copy(src, gr, f, ss.at[1 + p], up)])
            go((f > z) & has_down & most, [s_copy(src, gr, f, ss.at[1 + p], down)])
        most = None if most is True else most
        go(most, [s_copy(src, gr, f, sx.at[0], to_x)], False)
        go(most, [s_copy(src, gr, f, sy.at[0], to_y)], False)

    def shared_x(p):
        f = order[p]
        wait_shared(x_peer, f, tp)
        go(None, [s_copy(None, x_peer, f, sy.at[0], to_y)], False)

    def nt(a, b):
        return lax.dot_general(a, b, (((1,), (1,)), ((), ())), preferred_element_type=jnp.float32)

    def arrived(g, f):
        k = g * n_fs + f
        whole = w_all.at[k, c_other]
        remote(whole, whole, fs_.at[0], fr.at[k], to_c).wait_recv()

    def add(k, lo, hi, first):
        at = pl.ds(pl.multiple_of(k * cols, 128), cols)
        lhs = x_all[lo:hi, :, :, at].reshape((hi - lo) * rows, cols)
        here = slice(lo * rows, hi * rows)
        for s in range(n_tp):
            w = w_all[k, s // sides, s % sides, 0:2].reshape(2 * wide_hid, cols)
            val = nt(lhs, w)
            acc[s, here] = val if first else acc[s, here] + val

    def step(g, f, lo, hi, first=False):
        add(g * n_fs + f, lo, hi, first)

    def late(lo, hi):
        some = (hi - lo) * sub
        lhs = x_all[n_fs - 1, lo:hi].reshape(some, width)
        here = (n_fs - 1) * rows + lo * sub

        def one(s, carry):
            total = None
            for k in range(full):
                w = w_all[k, s // sides, s % sides, 0:2].reshape(2 * wide_hid, cols)
                val = nt(lhs[:, k * cols : (k + 1) * cols], w)
                total = val if total is None else total + val
            acc[s, here : here + some] = total
            return carry

        lax.fori_loop(0, n_tp, one, 0)

    def s_whole(t, i):
        return remote(s_slice(t), s_slice(t), sd.at[i], sc.at[t], to_c)

    s_results = [
        pltpu.make_async_copy(s_slice(tp).at[i], dst, res_sem.at[3 + i])
        for i, dst in enumerate((sg_hbm, su_hbm, sd_hbm))
    ]
    t_y = y_other * CORES + c

    def shared_give():
        near_s.wait()
        go(None, [s_whole(tp, 0)])
        for one in s_results:
            one.start()
        remote(s_slice(t_y), s_slice(t_y), sy.at[0], sr.at[full], to_y).wait_recv()
        go(None, [s_whole(t_y, 1)])

    def shared_act():
        for side in range(sides):
            s_whole(side * CORES + c_other, 0).wait_recv()
        lhs = x_all[0].reshape(rows, width)
        both = nt(lhs, s_all[0:2].reshape(2 * wide_hid, width))
        act[0] = (jax.nn.silu(both[:, :wide_hid]) * both[:, wide_hid:]).astype(jnp.bfloat16)

        def columns(k, inner):
            at = pl.ds(pl.multiple_of(k * cols, 128), cols)
            val = jnp.dot(act[0], s_all[2, :, at], preferred_element_type=jnp.float32)
            base[:, at] = val
            return inner

        lax.fori_loop(0, full, columns, 0)

    stages = []

    def then(f, *args):
        stages.append((f, args))

    def only(cond, f, *args):
        @functools.wraps(f)
        def run(*given):
            pl.when(cond)(lambda: f(*given))

        stages.append((run, args))

    def wide(v):
        return v.astype(jnp.float32)

    def u_copy(t, h):
        return remote(part.at[t, h], ru.at[t, h], us.at[t], cr.at[t, h], up)

    def d_copy(t, h, last_at=None):
        slot = jnp.where(t == (z - 1 if last_at is None else last_at), n_fs, t)
        return remote(part.at[t, h], rd.at[t, h], us.at[t], cr.at[slot, h], down)

    def when_way(t, ahead, behind):
        pl.when(t > z)(ahead)
        pl.when(t < z)(behind)

    def block(p, lo=0, hi=parts):
        t = order[p]
        some, skip = (hi - lo) * sub, lo * sub
        here = slice(p * rows + skip, p * rows + skip + some)

        for s in range(n_tp):
            e = z * n_tp + (s % sides) * CORES + s // sides
            scale = jnp.broadcast_to(t_all[t, pl.ds(e, 1), :], (rows, rows)).T
            scale = scale[skip : skip + some, :1]
            val = acc[s, here, :]
            val = jax.nn.silu(val[:, :wide_hid]) * val[:, wide_hid:] * scale
            act[s, 0:some] = val.astype(jnp.bfloat16)

        group = 8

        def columns(j, carry):
            for i in range(group):
                k = j * group + i
                at = pl.ds(pl.multiple_of(k * cols, 128), cols)
                total = None
                for s in range(n_tp):
                    val = jnp.dot(
                        act[s, 0:some], w_all[k, s // sides, s % sides, 2],
                        preferred_element_type=jnp.float32,
                    )
                    total = val if total is None else total + val
                total = total.astype(jnp.bfloat16)
                part[t, lo:hi, :, at] = total.reshape(hi - lo, sub, cols)
            return carry

        lax.fori_loop(0, full // group, columns, 0)
        if p:
            for g in range(lo, hi):
                pl.when((t > z) & jnp.logical_not(has_down))(lambda g=g: u_copy(t, g).start())
                pl.when((t < z) & jnp.logical_not(has_up))(lambda g=g: d_copy(t, g).start())

    def chain(p, lo=0, hi=parts):
        t = order[p]
        for h in range(lo, hi):
            for copy, arrived, cond in (
                (u_copy, ru, (t > z) & has_down), (d_copy, rd, (t < z) & has_up)
            ):

                @pl.when(cond)
                def _(h=h, copy=copy, arrived=arrived):
                    with jax.named_scope("chain"):
                        (u_copy(t, h) if copy is u_copy else d_copy(t, h, z)).wait_recv()
                    part[t, h] = (wide(part[t, h]) + wide(arrived[t, h])).astype(jnp.bfloat16)
                    copy(t, h).start()

    def mixed_copy(h):
        return pltpu.make_async_copy(mixed_out.at[h], mixed_hbm.at[h], loc.at[2 + h])

    def finish(h):
        mine_h = slice(h * sub, (h + 1) * sub)

        def total(*arrived):
            val = wide(part[z, h]) + base[mine_h, :]
            for one in arrived:
                val = val + wide(one)
            mixed_out[h] = val.astype(jnp.bfloat16)

        @pl.when(has_down & has_up)
        def _():
            u_copy(z, h).wait_recv()
            d_copy(z, h, z).wait_recv()
            total(ru[z, h], rd[z, h])

        @pl.when(jnp.logical_not(has_up))
        def _():
            u_copy(z, h).wait_recv()
            total(ru[z, h])

        @pl.when(jnp.logical_not(has_down))
        def _():
            d_copy(z, h, z).wait_recv()
            total(rd[z, h])

        mixed_copy(h).start()

    last, half_way = n_fs - 1, parts // 2
    then(own, 0, 1)
    then(own, 1, 0)
    then(own, 1, 1)
    then(side, 0, 0)
    then(side, 0, 1)
    then(column, 0)
    for p in range(2, n_fs):
        then(own, p, 0)
    then(side, 1, 0)
    then(side, 1, 1)
    then(column, 1)
    for p in range(2, n_fs):
        then(own, p, 1)
    for p in range(2, n_fs):
        then(side, p, 0)
    for h in range(half_way):
        then(row_part, 1, h, inner)
    then(row_part, 2, 0, inner)
    for h in range(half_way, parts):
        then(row_part, 1, h, inner)
    then(side, 2, 1)
    for h in range(1, parts - 1):
        then(row_part, 2, h, inner)
    then(side, last, 1)
    then(row_part, 2, parts - 1, inner)
    then(column, 2)
    then(column, last)
    then(corner, 0)
    then(corner, 1)
    for h in range(parts):
        then(row_part, 1, h, outer)
    then(shared, 0)
    then(shared, 1, outer)
    then(corner_turn, 0)
    then(corner_turn, 1)
    for p in range(n_fs):
        then(arrived, gr, order[p])
        then(step, gr, order[p], 0, 2, p == 0)
    for p in range(2):
        then(arrived, x_peer, order[p])
        then(step, x_peer, order[p], 0, 2)
    for h in range(half_way):
        then(row_part, last, h, inner)
    for h in range(parts):
        then(row_part, 2, h, outer)
    then(step, gr, order[0], 2, 3, True)
    then(step, gr, order[1], 2, 3)
    then(corner, 2)
    for h in range(half_way, parts - 1):
        then(row_part, last, h, inner)
    for p in range(2, n_fs):
        then(step, gr, order[p], 2, 3)
    then(row_part, last, parts - 1, inner)
    then(shared, 1, inner)
    then(shared, 2, inner)
    then(corner, last)
    for p in range(2):
        then(step, x_peer, order[p], 2, 3)
    for p in range(2, n_fs):
        then(arrived, x_peer, order[p])
        then(step, x_peer, order[p], 0, 3)
    then(block, last - 1)
    only(inner, chain, last - 1, 0, 1)
    only(inner, late, 0, parts)
    only(inner, chain, last - 1, 1, 2)
    only(inner, block, last, 0, parts)
    for lo, hi in ((0, half_way), (half_way, parts)):
        for h in range(lo, hi):
            then(row_part, last, h, outer)
        only(outer, late, lo, hi)
        only(outer, block, last, lo, hi)
    then(chain, last - 1, half_way, parts - 1)
    then(shared, last, inner)
    then(block, 1)
    then(chain, last - 1, parts - 1, parts)
    then(shared, 2, outer)
    then(block, 0)
    then(shared, last, outer)
    then(shared_x, 0)
    then(shared_x, 1)
    then(chain, last, 0, 1)
    then(corner_turn, 2)
    then(corner_turn, last)
    then(chain, last, 1, 2)
    then(shared_x, 2)
    then(shared_x, last)
    for h in range(2, parts):
        then(chain, 1, h - 2, h - 1)
        then(chain, last, h, h + 1)
    then(chain, 1, parts - 2, parts - 1)
    then(shared_give)
    then(chain, 1, parts - 1, parts)
    then(shared_act)
    for h in range(parts):
        then(finish, h)

    for f, args in stages:
        with jax.named_scope(f.__name__ + "_".join(str(a) for a in args if type(a) is int)):
            f(*args)

    with jax.named_scope("drain"):
        for h in range(parts):
            mixed_copy(h).wait()
        for one in s_results:
            one.wait()
        for i, (src, dst) in enumerate((
            (gate_out, gate_hbm), (up_out, up_hbm), (gate_out, gate_hbm),
        )):
            pltpu.make_async_copy(src, dst, res_sem.at[i]).wait()
        for cond, copies in pending:
            when(cond, lambda copies=copies: [one.wait_send() for one in copies] and None)
        for t in range(n_fs):
            whole = part.at[t]
            pl.when(t != z)(lambda: remote(whole, whole, us.at[t], cr.at[t, 0], to_c).wait_send())


def copy_kernel(count, *refs):
    ins, outs, sems = refs[:count], refs[count : 2 * count], refs[-1]
    copies = [pltpu.make_async_copy(ins[i], outs[i], sems.at[i]) for i in range(count)]
    for one in copies:
        one.start()
    for one in copies:
        one.wait()


def copied(arrays):
    count = len(arrays)
    return pl.pallas_call(
        functools.partial(copy_kernel, count),
        out_shape=tuple(jax.ShapeDtypeStruct(a.shape, a.dtype) for a in arrays),
        in_specs=[pl.BlockSpec(memory_space=pl.ANY)] * count,
        out_specs=(pl.BlockSpec(memory_space=pl.ANY),) * count,
        scratch_shapes=[pltpu.SemaphoreType.DMA((count,))],
        compiler_params=pltpu.CompilerParams(vmem_limit_bytes=COPY_LIMIT),
    )(*arrays)


def line_body(
    n_gr, n_fs, n_tp,
    prompt, train_gate, train_up, train_down, train_shared_gate, train_shared_up,
    train_shared_down, norm_gain, expert_ids, route_weight,
):
    experts, cols, hid = train_gate.shape
    rows, width = prompt.shape
    full, parts, sides = n_gr * n_fs, PARTS, n_tp // CORES
    sub, wide_hid = rows // parts, n_tp * hid
    bf16 = jnp.bfloat16
    f32 = jnp.float32
    hbm = pl.BlockSpec(memory_space=pl.ANY)
    dma = pltpu.SemaphoreType.DMA
    outs = pl.pallas_call(
        functools.partial(line_kernel, n_gr, n_fs, n_tp, parts),
        out_shape=(
            pltpu.VMEM((width, wide_hid), bf16),
            pltpu.VMEM((width, wide_hid), bf16),
            pltpu.VMEM((wide_hid, width), bf16),
            pltpu.VMEM((hid, width), bf16),
            pltpu.VMEM((hid, width), bf16),
            pltpu.VMEM((hid, width), bf16),
            pltpu.VMEM((parts, sub, width), bf16),
        ),
        in_specs=[hbm] * 10,
        out_specs=(hbm,) * 7,
        scratch_shapes=[
            pltpu.VMEM((rows, width), bf16),
            pltpu.VMEM((experts, hid, cols), f32),
            pltpu.VMEM((experts, hid, cols), f32),
            pltpu.VMEM((experts, hid, cols), f32),
            pltpu.VMEM((hid, cols), f32),
            pltpu.VMEM((hid, cols), f32),
            pltpu.VMEM((hid, cols), f32),
            pltpu.VMEM((1, cols), f32),
            pltpu.VMEM((expert_ids.shape[1], rows), jnp.int32),
            pltpu.VMEM((expert_ids.shape[1], rows), f32),
            pltpu.VMEM((n_fs, parts, sub, width), bf16),
            pltpu.VMEM((n_fs, experts, rows), f32),
            pltpu.VMEM((n_fs, CORES, sides, 3, hid, cols), bf16),
            pltpu.VMEM((full, CORES, sides, 3, wide_hid, cols), bf16),
            pltpu.VMEM((3, hid, cols), bf16),
            pltpu.VMEM((3, wide_hid, width), bf16),
            pltpu.VMEM((width, wide_hid), bf16),
            pltpu.VMEM((width, wide_hid), bf16),
            pltpu.VMEM((n_tp, n_fs * rows, 2 * wide_hid), f32),
            pltpu.VMEM((n_tp, rows, wide_hid), bf16),
            pltpu.VMEM((rows, width), f32),
            pltpu.VMEM((parts, sub, width), bf16),
            pltpu.VMEM((n_fs, parts, sub, width), bf16),
            pltpu.VMEM((n_fs, parts, sub, width), bf16),
            pltpu.VMEM((n_fs, parts, sub, width), bf16),
            dma((n_fs, parts)), dma((n_fs,)), dma((full * n_tp,)), dma((full + 1,)),
            dma((n_tp,)), dma((full,)), dma((n_fs + 1, parts)),
            dma((3,)), dma((n_fs + 1, 2)), dma((1,)), dma((1,)), dma((1,)), dma((1,)),
            dma((1,)), dma((n_fs + 1,)), dma((1,)), dma((1,)), dma((2,)),
            dma((n_fs,)),
            dma((2 + parts,)), dma((6,)), dma((7 + n_fs,)),
        ],
        compiler_params=pltpu.CompilerParams(
            collective_id=0, has_side_effects=True, vmem_limit_bytes=VMEM_LIMIT
        ),
    )(
        prompt, train_gate.transpose(0, 2, 1), train_up.transpose(0, 2, 1), train_down,
        train_shared_gate.T, train_shared_up.T, train_shared_down, norm_gain[None, :],
        expert_ids.T, route_weight.T,
    )
    serve_gate, serve_up, serve_down, s_gate, s_up, s_down, mixed_out = copied(outs)
    return (
        serve_gate[None], serve_up[None], serve_down[None],
        s_gate.T, s_up.T, s_down, mixed_out.reshape(rows, width),
    )


def regroup(stacked, lowered):
    stacked = lax.all_to_all(
        lax.all_to_all(stacked, "fs", split_axis=0, concat_axis=2, tiled=True),
        "tp",
        split_axis=0,
        concat_axis=3,
        tiled=True,
    )
    lowered = lax.all_to_all(
        lax.all_to_all(lowered, "fs", split_axis=0, concat_axis=2, tiled=True),
        "tp",
        split_axis=0,
        concat_axis=1,
        tiled=True,
    )
    return (stacked, lowered)


def body(
    prompt,
    train_gate,
    train_up,
    train_down,
    train_shared_gate,
    train_shared_up,
    train_shared_down,
    norm_gain,
    expert_ids,
    route_weight,
):
    gain_col = norm_gain[:, None]
    stacked = jnp.stack((train_gate * gain_col[None], train_up * gain_col[None]), axis=1).astype(
        jnp.bfloat16
    )
    lowered = train_down.astype(jnp.bfloat16)
    stacked, lowered = regroup(stacked, lowered)
    stacked, lowered = (
        lax.all_gather(stacked, "gr", axis=2, tiled=True),
        lax.all_gather(lowered, "gr", axis=2, tiled=True),
    )
    serve_gate = stacked[:, 0]
    serve_up = stacked[:, 1]
    serve_shared_gate, serve_shared_up, serve_shared_down = (
        lax.all_gather(
            (train_shared_gate * gain_col).astype(jnp.bfloat16), ("gr", "fs"), axis=0, tiled=True
        ),
        lax.all_gather(
            (train_shared_up * gain_col).astype(jnp.bfloat16), ("gr", "fs"), axis=0, tiled=True
        ),
        lax.all_gather(train_shared_down.astype(jnp.bfloat16), ("gr", "fs"), axis=1, tiled=True),
    )
    widened = prompt.astype(jnp.float32)
    normed = (
        widened * lax.rsqrt(jnp.mean(widened * widened, axis=-1, keepdims=True) + eps_norm)
    ).astype(jnp.bfloat16)
    block_rows = lax.all_gather(normed, "tp", axis=0, tiled=True)
    gate_val = jnp.dot(block_rows, serve_shared_gate, preferred_element_type=jnp.float32)
    up_val = jnp.dot(block_rows, serve_shared_up, preferred_element_type=jnp.float32)
    shared_act = (jax.nn.silu(gate_val) * up_val).astype(jnp.bfloat16)
    shared_sum = lax.psum_scatter(
        jnp.dot(shared_act, serve_shared_down, preferred_element_type=jnp.float32).astype(
            jnp.bfloat16
        ),
        "tp",
        scatter_dimension=0,
        tiled=True,
    ).astype(jnp.float32)
    row_count = prompt.shape[0]
    top_count = expert_ids.shape[1]
    model_width = prompt.shape[1]
    expert_count = lax.axis_size("fs") * lax.axis_size("tp")
    capacity = row_count * top_count // expert_count + 1
    flat_ids = expert_ids.reshape(-1)
    onehot = (flat_ids[:, None] == jnp.arange(expert_count, dtype=jnp.int32)[None, :]).astype(
        jnp.int32
    )
    earlier = jnp.cumsum(onehot, axis=0) - onehot
    places = jnp.sum(earlier * onehot, axis=1)
    slot_ids = (flat_ids * capacity + places).reshape(row_count, top_count)
    slot_range = jnp.arange(expert_count * capacity, dtype=jnp.int32)
    dispatch = jnp.any(slot_range[:, None, None] == slot_ids[None, :, :], axis=-1).astype(
        jnp.bfloat16
    )
    outgoing = jnp.dot(dispatch, normed, preferred_element_type=jnp.float32).astype(jnp.bfloat16)
    outgoing = outgoing.reshape(expert_count, capacity, model_width)
    arrived = lax.all_to_all(outgoing, ("fs", "tp"), split_axis=0, concat_axis=0, tiled=True)
    source_count, slot_count, width_here = arrived.shape
    arrived_rows = arrived.reshape(source_count * slot_count, width_here)
    gate_val = jnp.dot(arrived_rows, serve_gate[0], preferred_element_type=jnp.float32)
    up_val = jnp.dot(arrived_rows, serve_up[0], preferred_element_type=jnp.float32)
    hidden = (jax.nn.silu(gate_val) * up_val).astype(jnp.bfloat16)
    result = jnp.dot(hidden, lowered[0], preferred_element_type=jnp.float32).astype(jnp.bfloat16)
    result = result.reshape(source_count, slot_count, width_here)
    returned = lax.all_to_all(result, ("fs", "tp"), split_axis=0, concat_axis=0, tiled=True)
    picked = returned.reshape(expert_count * capacity, model_width)[slot_ids]
    routed = jnp.sum(route_weight[:, :, None] * picked.astype(jnp.float32), axis=1)
    mixed_out = (routed + shared_sum).astype(jnp.bfloat16)
    return (
        serve_gate,
        serve_up,
        lowered,
        serve_shared_gate,
        serve_shared_up,
        serve_shared_down,
        mixed_out,
    )


def solution(mesh):
    placed = (
        P(("gr", "fs", "tp"), None),
        P(None, ("gr", "fs"), "tp"),
        P(None, ("gr", "fs"), "tp"),
        P(None, "tp", ("gr", "fs")),
        P(("gr", "fs"), "tp"),
        P(("gr", "fs"), "tp"),
        P("tp", ("gr", "fs")),
        P(("gr", "fs")),
        P(("gr", "fs", "tp"), None),
        P(("gr", "fs", "tp"), None),
    )
    n_gr, n_fs, n_tp = (mesh.shape[name] for name in ("gr", "fs", "tp"))

    def chosen(prompt, train_gate, *rest):
        rows, width = prompt.shape
        experts, cols, hid = train_gate.shape
        held = n_fs * n_tp * n_gr * CORES * 3 * hid * cols * 4 + 4 * n_fs * prompt.size * 2
        fits = n_gr == 2 and n_tp == 2 * CORES and n_fs % 2 == 0 and held < VMEM_PLAN
        even = experts == n_fs * n_tp and cols * n_gr * n_fs == width and rows == 128
        if fits and even and hid % (16 * n_fs) == 0 and cols % 128 == 0:
            return line_body(n_gr, n_fs, n_tp, prompt, train_gate, *rest)
        return body(prompt, train_gate, *rest)

    return jax.shard_map(
        chosen,
        mesh=mesh,
        in_specs=placed,
        out_specs=(
            P(("fs", "tp"), None, None),
            P(("fs", "tp"), None, None),
            P(("fs", "tp"), None, None),
            P(None, "tp"),
            P(None, "tp"),
            P("tp", None),
            P(("gr", "fs", "tp"), None),
        ),
        check_vma=False,
    )
```

```python
import functools

import jax
import jax.numpy as jnp
from jax import lax
from jax.experimental import pallas as pl
from jax.experimental.pallas import tpu as pltpu
from jax.sharding import PartitionSpec as P

eps_norm = 1e-06
MESH = pl.DeviceIdType.MESH
CORES = 2
PARTS = 4
VMEM_PLAN = 40 * 2**20
VMEM_LIMIT = 119 * 2**19
COPY_LIMIT = 4 * 2**20


def line_kernel(
    n_gr, n_fs, n_tp, parts,
    p_hbm, gt_hbm, ut_hbm, dn_hbm, tsg_hbm, tsu_hbm, tsd_hbm, gain_hbm, ids_hbm, rw_hbm,
    gate_hbm, up_hbm, down_hbm, sg_hbm, su_hbm, sd_hbm, mixed_hbm,
    p_ref, gt_ref, ut_ref, dn_ref, sg_ref, su_ref, sd_ref, gain_ref, ids_ref, rw_ref,
    x_all, t_all, e_in, w_all, s_in, s_all, gate_out, up_out, acc, act, base, mixed_out,
    part, ru, rd,
    xr, tr, er, sr, sc, fr, cr,
    zs, zd, xs, ys, xd, yd, fs_, ss, sx, sy, sd, us, loc, res_sem, in_sem,
):
    gr, z, tp = lax.axis_index("gr"), lax.axis_index("fs"), lax.axis_index("tp")
    y, c = tp // CORES, tp % CORES
    sides = n_tp // CORES
    x_peer, y_other, c_other = 1 - gr, 1 - y, 1 - c
    _, hid, cols = s_in.shape
    sub, width = x_all.shape[2], x_all.shape[3]
    rows = parts * sub
    full = n_gr * n_fs
    wide_hid = n_tp * hid

    def dev(g, f, t):
        return {"gr": g, "fs": f, "tp": t}

    to_x, to_y = dev(x_peer, z, tp), dev(gr, z, y_other * CORES + c)
    to_c = dev(gr, z, y * CORES + c_other)
    up, down = dev(gr, z + 1, tp), dev(gr, z - 1, tp)
    has_up, has_down = z < n_fs - 1, z > 0
    inner = has_up & has_down
    outer = jnp.logical_not(inner)

    def far(p):
        if p == n_fs - 1:
            return z
        fall, rise = n_fs - 1 - p, p
        fall = jnp.where(fall <= z, fall - 1, fall)
        rise = jnp.where(rise >= z, rise + 1, rise)
        return jnp.where(z < n_fs // 2, fall, rise)

    order = [far(n_fs - 1 - p) for p in range(n_fs)]

    def place(f, at):
        rise = jnp.where(f < at, f + 1, f)
        fall = jnp.where(f > at, n_fs - f, n_fs - 1 - f)
        return jnp.where(f == at, 0, jnp.where(at < n_fs // 2, rise, fall))

    barrier = pltpu.get_barrier_semaphore()

    def greet(where):
        pl.semaphore_signal(barrier, inc=1, device_id=where, device_id_type=MESH)

    for dz in range(n_fs):
        for dc in range(CORES):
            if dz or dc:
                greet(dev(gr, (z + dz) % n_fs, y * CORES + (c + dc) % CORES))
    greet(to_x)
    greet(to_y)

    first = pltpu.make_async_copy(gain_hbm, gain_ref, in_sem.at[0])
    first.start()
    heavy = []
    for p in range(n_fs):
        at = pl.ds(order[p] * n_tp, n_tp)
        heavy.append([
            pltpu.make_async_copy(src.at[at], dst.at[at], in_sem.at[1 + p])
            for src, dst in ((gt_hbm, gt_ref), (ut_hbm, ut_ref), (dn_hbm, dn_ref))
        ])
    light = [
        pltpu.make_async_copy(src, dst, in_sem.at[1 + n_fs + i])
        for i, (src, dst) in enumerate((
            (tsg_hbm, sg_ref), (tsu_hbm, su_ref), (tsd_hbm, sd_ref), (p_hbm, p_ref),
            (ids_hbm, ids_ref), (rw_hbm, rw_ref),
        ))
    ]
    for one in sum(heavy, []) + light:
        one.start()

    first.wait()
    gain = gain_ref[...]

    def cast(p):
        all_of = pl.ds(0, 3 * n_tp)
        pltpu.make_async_copy(gt_hbm.at[all_of], gt_ref.at[all_of], in_sem.at[1 + p]).wait()
        f = order[p]
        for t in range(n_tp):
            i = f * n_tp + t
            e_in[f, t % CORES, t // CORES, 0] = (gt_ref[i] * gain).astype(jnp.bfloat16)
            e_in[f, t % CORES, t // CORES, 1] = (ut_ref[i] * gain).astype(jnp.bfloat16)
            e_in[f, t % CORES, t // CORES, 2] = dn_ref[i].astype(jnp.bfloat16)

    with jax.named_scope("cast0"):
        cast(0)
    with jax.named_scope("greeted"):
        pl.semaphore_wait(barrier, n_fs * CORES + 1)

    def remote(src, dst, send, recv, where):
        return pltpu.make_async_remote_copy(
            src_ref=src, dst_ref=dst, send_sem=send, recv_sem=recv,
            device_id=where, device_id_type=MESH,
        )

    pending = []

    def when(cond, f):
        if cond is None:
            f()
        else:
            pl.when(cond)(f)

    def go(cond, copies, drain=True):
        if drain:
            pending.append((cond, copies))

        def start():
            for one in copies:
                one.start()

        when(cond, start)

    def drain(cond, ref, sem):
        pending.append((cond, [remote(ref, ref, sem, sc.at[0], to_c)]))

    def slab(g, f, t, core):
        at = pl.ds(pl.multiple_of(t * hid, hid), hid)
        return w_all.at[g * n_fs + f, core, :, :, at, :]

    def got(g, f, t):
        return er.at[(g * n_fs + f) * n_tp + t]

    def send_expert(p, i):
        f = order[p]
        core = c if i == 0 else c_other
        go(None, [remote(
            e_in.at[f, core], slab(gr, z, tp, core), zs.at[1 if p == 1 else 2],
            got(gr, z, tp), dev(gr, f, y * CORES + core),
        )], False)

    def wait_slab(g, f, t):
        remote(e_in.at[0, 0], slab(g, f, t, c), zs.at[0], got(g, f, t), to_x).wait_recv()

    def pass_slab(g, f, t, sem, where, src=None):
        place = slab(g, f, t, c)
        return remote(place if src is None else src, place, sem, got(g, f, t), where)

    def send_rows(cond, f, h, slot, way):
        to = z + 1 if way == 0 else z - 1
        here, there = place(f, z), place(f, to)
        where = dev(gr, to, tp)
        sem = zd.at[slot, 0]
        go(cond, [remote(x_all.at[here, h], x_all.at[there, h], sem, xr.at[f, h], where)], False)
        if h == 0:
            drain(cond, x_all.at[0], sem)
            go(cond, [remote(t_all.at[f], t_all.at[f], zd.at[slot, 1], tr.at[f], where)])

    def s_slice(t):
        return s_all.at[:, pl.ds(pl.multiple_of(t * hid, hid), hid), :]

    def s_slab(g, f, t):
        lanes = pl.ds(pl.multiple_of((g * n_fs + f) * cols, 128), cols)
        return s_all.at[:, pl.ds(pl.multiple_of(t * hid, hid), hid), lanes]

    def s_copy(src, g, f, sem, where, t=tp):
        src = s_slab(g, f, t) if src is None else src
        recv = sr.at[full] if where is to_y else sr.at[g * n_fs + f]
        return remote(src, s_slab(g, f, t), sem, recv, where)

    mine = e_in.at[z, c]
    go(None, [remote(
        e_in.at[z, c_other], slab(gr, z, tp, c_other), zs.at[0], got(gr, z, tp), to_c
    )])
    go(None, [pass_slab(gr, z, tp, xs.at[0], to_x, mine)], False)
    go(None, [pass_slab(gr, z, tp, ys.at[0], to_y, mine)], False)
    cast(1)
    for i in range(CORES):
        send_expert(1, i)
    for p in range(2, n_fs):
        cast(p)
    for i in range(CORES):
        for p in range(2, n_fs):
            send_expert(p, i)
    drain(None, w_all.at[0, 0, 0], zs.at[1])
    drain(None, w_all.at[0, 0], zs.at[2])
    drain(None, w_all.at[0], xs.at[0])
    drain(None, w_all.at[0], ys.at[0])
    drain(None, w_all.at[0, 0], xd.at[0])
    drain(None, w_all.at[0, 0], yd.at[0])
    drain(None, w_all.at[0 : full // 2], fs_.at[0])
    drain(None, w_all.at[0, 0, 0], sx.at[0])
    drain(None, s_slice(tp), sy.at[0])
    near_slab = pltpu.make_async_copy(mine, slab(gr, z, tp, c), loc.at[0])
    near_slab.start()

    for one in light:
        one.wait()
    s_in[0] = (sg_ref[...] * gain).astype(jnp.bfloat16)
    s_in[1] = (su_ref[...] * gain).astype(jnp.bfloat16)
    s_in[2] = sd_ref[...].astype(jnp.bfloat16)
    for h in range(parts):
        v = p_ref[h * sub : (h + 1) * sub, :].astype(jnp.float32)
        mean = jnp.mean(v * v, axis=-1, keepdims=True)
        x_all[0, h] = (v * lax.rsqrt(mean + eps_norm)).astype(jnp.bfloat16)
    shape = t_all.shape[1:]
    table = jnp.zeros(shape, jnp.float32)
    which = lax.broadcasted_iota(jnp.int32, shape, 0)
    for k in range(ids_ref.shape[0]):
        table = table + jnp.where(ids_ref[k : k + 1, :] == which, rw_ref[k : k + 1, :], 0.0)
    t_all[z] = table

    near_s = pltpu.make_async_copy(s_in, s_slab(gr, z, tp), loc.at[1])
    near_s.start()

    def send_own(cond):
        for h in range(parts):
            for way in (0, 1):
                there = has_up if way == 0 else has_down
                send_rows(there & cond, z, h, way, way)
        go(has_up & cond, [s_copy(s_in, gr, z, ss.at[0], up)])
        go(has_down & cond, [s_copy(s_in, gr, z, ss.at[1], down)])

    send_own(True)

    def own(p, i):
        f = order[p]
        core = c if i == 0 else c_other
        t = y * CORES + core
        wait_slab(gr, f, t)
        go(None, [pass_slab(gr, f, t, xs.at[0], to_x)], False)
        go(None, [pass_slab(gr, f, t, ys.at[0], to_y)], False)

    def result_copies(k):
        at = pl.ds(pl.multiple_of(k * cols, 128), cols)
        return [
            pltpu.make_async_copy(gate_out.at[at, :], gate_hbm.at[at, :], res_sem.at[0]),
            pltpu.make_async_copy(up_out.at[at, :], up_hbm.at[at, :], res_sem.at[1]),
            pltpu.make_async_copy(w_all.at[k, c, y, 2], down_hbm.at[:, at], res_sem.at[2]),
        ]

    half = wide_hid // sides

    def half_copy(k, core, part_of):
        at = pl.ds(pl.multiple_of(part_of * half, half), half)
        place_of = w_all.at[k, core, :, :, at, :]
        return remote(place_of, place_of, fs_.at[0], fr.at[k], to_c)

    def give(g, f, part_of):
        go(None, [half_copy(g * n_fs + f, c, part_of)], False)

    def turn(g, f):
        k = g * n_fs + f
        at = pl.ds(pl.multiple_of(k * cols, 128), cols)
        gate_out[at, :] = w_all[k, c, y, 0].T
        up_out[at, :] = w_all[k, c, y, 1].T
        for one in result_copies(k):
            one.start()

    def side(p, i):
        f = order[p]
        core = c if i == 0 else c_other
        wait_slab(x_peer, f, y * CORES + core)
        if (p + i) % 2 == 0:
            go(None, [pass_slab(x_peer, f, y * CORES + core, yd.at[0], to_y)], False)
        wait_slab(gr, f, y_other * CORES + core)
        if (p + i) % 2 == 1:
            go(None, [pass_slab(gr, f, y_other * CORES + core, xd.at[0], to_x)], False)
        if i == CORES - 1:
            give(x_peer, f, y)

    def column(p):
        if p == 0:
            near_slab.wait()
        give(gr, order[p], y)
        give(gr, order[p], y_other)
        turn(gr, order[p])

    def corner(p):
        f = order[p]
        for core in range(CORES):
            wait_slab(x_peer, f, y_other * CORES + core)
        give(x_peer, f, y_other)

    def corner_turn(p):
        turn(x_peer, order[p])

    def row_part(p, h, most=None):
        f = order[p]

        def arrive():
            remote(x_all.at[p, h], x_all.at[p, h], zd.at[0, 0], xr.at[f, h], to_x).wait_recv()
            if h == 0:
                remote(t_all.at[f], t_all.at[f], zd.at[0, 0], tr.at[f], to_x).wait_recv()

        when(most, arrive)
        if most is inner:
            send_rows((f < z) & inner, f, h, 1 + p, 0)
            send_rows((f > z) & inner, f, h, 1 + p, 1)

    def wait_shared(g, f, t):
        s_copy(None, g, f, sx.at[0], to_x, t).wait_recv()

    def shared(p, most=True):
        f = order[p]
        src = None if p else s_in
        if p:
            when(None if most is True else most, functools.partial(wait_shared, gr, f, tp))
            go((f < z) & has_up & most, [s_copy(src, gr, f, ss.at[1 + p], up)])
            go((f > z) & has_down & most, [s_copy(src, gr, f, ss.at[1 + p], down)])
        most = None if most is True else most
        go(most, [s_copy(src, gr, f, sx.at[0], to_x)], False)
        go(most, [s_copy(src, gr, f, sy.at[0], to_y)], False)

    def shared_x(p):
        f = order[p]
        wait_shared(x_peer, f, tp)
        go(None, [s_copy(None, x_peer, f, sy.at[0], to_y)], False)

    def nt(a, b):
        return lax.dot_general(a, b, (((1,), (1,)), ((), ())), preferred_element_type=jnp.float32)

    def arrived(g, f):
        k = g * n_fs + f
        whole = w_all.at[k, c_other]
        remote(whole, whole, fs_.at[0], fr.at[k], to_c).wait_recv()

    def add(k, lo, hi, first, cores):
        at = pl.ds(pl.multiple_of(k * cols, 128), cols)
        lhs = x_all[lo:hi, :, :, at].reshape((hi - lo) * rows, cols)
        here = slice(lo * rows, hi * rows)
        for core in cores:
            for side_of in range(sides):
                s = core * sides + side_of
                w = w_all[k, core, side_of, 0:2].reshape(2 * wide_hid, cols)
                val = nt(lhs, w)
                acc[s, here] = val if first else acc[s, here] + val

    def step(g, f, lo, hi, first=False):
        add(g * n_fs + f, lo, hi, first, range(CORES))

    def step_of(g, f, core):
        add(g * n_fs + f, 0, n_fs - 1, False, (core,))

    def late(lo, hi):
        some = (hi - lo) * sub
        lhs = x_all[n_fs - 1, lo:hi].reshape(some, width)
        here = (n_fs - 1) * rows + lo * sub

        def one(s, carry):
            total = None
            for k in range(full):
                w = w_all[k, s // sides, s % sides, 0:2].reshape(2 * wide_hid, cols)
                val = nt(lhs[:, k * cols : (k + 1) * cols], w)
                total = val if total is None else total + val
            acc[s, here : here + some] = total
            return carry

        lax.fori_loop(0, n_tp, one, 0)

    def s_whole(t, i):
        return remote(s_slice(t), s_slice(t), sd.at[i], sc.at[t], to_c)

    s_results = [
        pltpu.make_async_copy(s_slice(tp).at[i], dst, res_sem.at[3 + i])
        for i, dst in enumerate((sg_hbm, su_hbm, sd_hbm))
    ]
    t_y = y_other * CORES + c

    def shared_give():
        near_s.wait()
        go(None, [s_whole(tp, 0)])
        for one in s_results:
            one.start()
        remote(s_slice(t_y), s_slice(t_y), sy.at[0], sr.at[full], to_y).wait_recv()
        go(None, [s_whole(t_y, 1)])

    def shared_act():
        for side in range(sides):
            s_whole(side * CORES + c_other, 0).wait_recv()
        lhs = x_all[0].reshape(rows, width)
        both = nt(lhs, s_all[0:2].reshape(2 * wide_hid, width))
        act[0] = (jax.nn.silu(both[:, :wide_hid]) * both[:, wide_hid:]).astype(jnp.bfloat16)

        def columns(k, inner):
            at = pl.ds(pl.multiple_of(k * cols, 128), cols)
            val = jnp.dot(act[0], s_all[2, :, at], preferred_element_type=jnp.float32)
            base[:, at] = val
            return inner

        lax.fori_loop(0, full, columns, 0)

    stages = []

    def then(f, *args):
        stages.append((f, args))

    def only(cond, f, *args):
        @functools.wraps(f)
        def run(*given):
            pl.when(cond)(lambda: f(*given))

        stages.append((run, args))

    def wide(v):
        return v.astype(jnp.float32)

    def u_copy(t, h):
        return remote(part.at[t, h], ru.at[t, h], us.at[t], cr.at[t, h], up)

    def d_copy(t, h, last_at=None):
        slot = jnp.where(t == (z - 1 if last_at is None else last_at), n_fs, t)
        return remote(part.at[t, h], rd.at[t, h], us.at[t], cr.at[slot, h], down)

    def when_way(t, ahead, behind):
        pl.when(t > z)(ahead)
        pl.when(t < z)(behind)

    def block(p, lo=0, hi=parts):
        t = order[p]
        some, skip = (hi - lo) * sub, lo * sub
        here = slice(p * rows + skip, p * rows + skip + some)

        for s in range(n_tp):
            e = z * n_tp + (s % sides) * CORES + s // sides
            scale = jnp.broadcast_to(t_all[t, pl.ds(e, 1), :], (rows, rows)).T
            scale = scale[skip : skip + some, :1]
            val = acc[s, here, :]
            val = jax.nn.silu(val[:, :wide_hid]) * val[:, wide_hid:] * scale
            act[s, 0:some] = val.astype(jnp.bfloat16)

        group = 8

        def columns(j, carry):
            for i in range(group):
                k = j * group + i
                at = pl.ds(pl.multiple_of(k * cols, 128), cols)
                total = None
                for s in range(n_tp):
                    val = jnp.dot(
                        act[s, 0:some], w_all[k, s // sides, s % sides, 2],
                        preferred_element_type=jnp.float32,
                    )
                    total = val if total is None else total + val
                total = total.astype(jnp.bfloat16)
                part[t, lo:hi, :, at] = total.reshape(hi - lo, sub, cols)
            return carry

        lax.fori_loop(0, full // group, columns, 0)
        if p:
            for g in range(lo, hi):
                pl.when((t > z) & jnp.logical_not(has_down))(lambda g=g: u_copy(t, g).start())
                pl.when((t < z) & jnp.logical_not(has_up))(lambda g=g: d_copy(t, g).start())

    def chain(p, lo=0, hi=parts):
        t = order[p]
        for h in range(lo, hi):
            for copy, arrived, cond in (
                (u_copy, ru, (t > z) & has_down), (d_copy, rd, (t < z) & has_up)
            ):

                @pl.when(cond)
                def _(h=h, copy=copy, arrived=arrived):
                    with jax.named_scope("chain"):
                        (u_copy(t, h) if copy is u_copy else d_copy(t, h, z)).wait_recv()
                    part[t, h] = (wide(part[t, h]) + wide(arrived[t, h])).astype(jnp.bfloat16)
                    copy(t, h).start()

    def mixed_copy(h):
        return pltpu.make_async_copy(mixed_out.at[h], mixed_hbm.at[h], loc.at[2 + h])

    def finish(h):
        mine_h = slice(h * sub, (h + 1) * sub)

        def total(*arrived):
            val = wide(part[z, h]) + base[mine_h, :]
            for one in arrived:
                val = val + wide(one)
            mixed_out[h] = val.astype(jnp.bfloat16)

        @pl.when(has_down & has_up)
        def _():
            u_copy(z, h).wait_recv()
            d_copy(z, h, z).wait_recv()
            total(ru[z, h], rd[z, h])

        @pl.when(jnp.logical_not(has_up))
        def _():
            u_copy(z, h).wait_recv()
            total(ru[z, h])

        @pl.when(jnp.logical_not(has_down))
        def _():
            d_copy(z, h, z).wait_recv()
            total(rd[z, h])

        mixed_copy(h).start()

    last, half_way = n_fs - 1, parts // 2
    then(own, 0, 1)
    then(own, 1, 0)
    then(own, 1, 1)
    then(side, 0, 0)
    then(side, 0, 1)
    then(column, 0)
    for p in range(2, n_fs):
        then(own, p, 0)
    then(side, 1, 0)
    then(side, 1, 1)
    then(column, 1)
    for p in range(2, n_fs):
        then(own, p, 1)
    for p in range(2, n_fs):
        then(side, p, 0)
    for h in range(half_way):
        then(row_part, 1, h, inner)
    then(row_part, 2, 0, inner)
    for h in range(half_way, parts):
        then(row_part, 1, h, inner)
    then(side, 2, 1)
    for h in range(1, parts - 1):
        then(row_part, 2, h, inner)
    then(side, last, 1)
    then(row_part, 2, parts - 1, inner)
    then(column, 2)
    then(column, last)
    then(corner, 0)
    then(corner, 1)
    for h in range(parts):
        then(row_part, 1, h, outer)
    then(corner_turn, 0)
    then(corner_turn, 1)
    for p in range(n_fs):
        then(arrived, gr, order[p])
        then(step, gr, order[p], 0, 2, p == 0)
    for p in range(2):
        then(arrived, x_peer, order[p])
        then(step, x_peer, order[p], 0, 2)
    for h in range(half_way):
        then(row_part, last, h, inner)
    for h in range(parts):
        then(row_part, 2, h, outer)
    then(step, gr, order[0], 2, 3, True)
    then(step, gr, order[1], 2, 3)
    then(corner, 2)
    then(row_part, last, 2, inner)
    then(corner, last)
    for p in range(2, n_fs):
        then(step, gr, order[p], 2, 3)
    for p in range(2):
        then(step, x_peer, order[p], 2, 3)
    for p in range(2, n_fs):
        then(step_of, x_peer, order[p], c)
    then(row_part, last, parts - 1, inner)
    for p in range(2, n_fs):
        then(arrived, x_peer, order[p])
        then(step_of, x_peer, order[p], c_other)
    then(block, last - 1)
    then(shared, 0)
    then(shared, 1)
    then(shared, 2, inner)
    only(inner, chain, last - 1, 0, 1)
    only(inner, late, 0, parts)
    only(inner, chain, last - 1, 1, 2)
    only(inner, block, last, 0, parts)
    for lo, hi in ((0, half_way), (half_way, parts)):
        for h in range(lo, hi):
            then(row_part, last, h, outer)
        only(outer, late, lo, hi)
        only(outer, block, last, lo, hi)
    then(chain, last - 1, half_way, parts - 1)
    then(shared, last, inner)
    then(block, 1)
    then(chain, last - 1, parts - 1, parts)
    then(shared, 2, outer)
    then(block, 0)
    then(shared, last, outer)
    then(shared_x, 0)
    then(shared_x, 1)
    then(chain, last, 0, 1)
    then(corner_turn, 2)
    then(corner_turn, last)
    then(chain, last, 1, 2)
    then(shared_x, 2)
    then(shared_x, last)
    for h in range(2, parts):
        then(chain, 1, h - 2, h - 1)
        then(chain, last, h, h + 1)
    then(chain, 1, parts - 2, parts - 1)
    then(shared_give)
    then(chain, 1, parts - 1, parts)
    then(shared_act)
    for h in range(parts):
        then(finish, h)

    for f, args in stages:
        with jax.named_scope(f.__name__ + "_".join(str(a) for a in args if type(a) is int)):
            f(*args)

    with jax.named_scope("drain"):
        for h in range(parts):
            mixed_copy(h).wait()
        for one in s_results:
            one.wait()
        for i, (src, dst) in enumerate((
            (gate_out, gate_hbm), (up_out, up_hbm), (gate_out, gate_hbm),
        )):
            pltpu.make_async_copy(src, dst, res_sem.at[i]).wait()
        for cond, copies in pending:
            when(cond, lambda copies=copies: [one.wait_send() for one in copies] and None)
        for t in range(n_fs):
            whole = part.at[t]
            pl.when(t != z)(lambda: remote(whole, whole, us.at[t], cr.at[t, 0], to_c).wait_send())


def copy_kernel(count, *refs):
    ins, outs, sems = refs[:count], refs[count : 2 * count], refs[-1]
    copies = [pltpu.make_async_copy(ins[i], outs[i], sems.at[i]) for i in range(count)]
    for one in copies:
        one.start()
    for one in copies:
        one.wait()


def copied(arrays):
    count = len(arrays)
    return pl.pallas_call(
        functools.partial(copy_kernel, count),
        out_shape=tuple(jax.ShapeDtypeStruct(a.shape, a.dtype) for a in arrays),
        in_specs=[pl.BlockSpec(memory_space=pl.ANY)] * count,
        out_specs=(pl.BlockSpec(memory_space=pl.ANY),) * count,
        scratch_shapes=[pltpu.SemaphoreType.DMA((count,))],
        compiler_params=pltpu.CompilerParams(vmem_limit_bytes=COPY_LIMIT),
    )(*arrays)


def line_body(
    n_gr, n_fs, n_tp,
    prompt, train_gate, train_up, train_down, train_shared_gate, train_shared_up,
    train_shared_down, norm_gain, expert_ids, route_weight,
):
    experts, cols, hid = train_gate.shape
    rows, width = prompt.shape
    full, parts, sides = n_gr * n_fs, PARTS, n_tp // CORES
    sub, wide_hid = rows // parts, n_tp * hid
    bf16 = jnp.bfloat16
    f32 = jnp.float32
    hbm = pl.BlockSpec(memory_space=pl.ANY)
    dma = pltpu.SemaphoreType.DMA
    outs = pl.pallas_call(
        functools.partial(line_kernel, n_gr, n_fs, n_tp, parts),
        out_shape=(
            pltpu.VMEM((width, wide_hid), bf16),
            pltpu.VMEM((width, wide_hid), bf16),
            pltpu.VMEM((wide_hid, width), bf16),
            pltpu.VMEM((hid, width), bf16),
            pltpu.VMEM((hid, width), bf16),
            pltpu.VMEM((hid, width), bf16),
            pltpu.VMEM((parts, sub, width), bf16),
        ),
        in_specs=[hbm] * 10,
        out_specs=(hbm,) * 7,
        scratch_shapes=[
            pltpu.VMEM((rows, width), bf16),
            pltpu.VMEM((experts, hid, cols), f32),
            pltpu.VMEM((experts, hid, cols), f32),
            pltpu.VMEM((experts, hid, cols), f32),
            pltpu.VMEM((hid, cols), f32),
            pltpu.VMEM((hid, cols), f32),
            pltpu.VMEM((hid, cols), f32),
            pltpu.VMEM((1, cols), f32),
            pltpu.VMEM((expert_ids.shape[1], rows), jnp.int32),
            pltpu.VMEM((expert_ids.shape[1], rows), f32),
            pltpu.VMEM((n_fs, parts, sub, width), bf16),
            pltpu.VMEM((n_fs, experts, rows), f32),
            pltpu.VMEM((n_fs, CORES, sides, 3, hid, cols), bf16),
            pltpu.VMEM((full, CORES, sides, 3, wide_hid, cols), bf16),
            pltpu.VMEM((3, hid, cols), bf16),
            pltpu.VMEM((3, wide_hid, width), bf16),
            pltpu.VMEM((width, wide_hid), bf16),
            pltpu.VMEM((width, wide_hid), bf16),
            pltpu.VMEM((n_tp, n_fs * rows, 2 * wide_hid), f32),
            pltpu.VMEM((n_tp, rows, wide_hid), bf16),
            pltpu.VMEM((rows, width), f32),
            pltpu.VMEM((parts, sub, width), bf16),
            pltpu.VMEM((n_fs, parts, sub, width), bf16),
            pltpu.VMEM((n_fs, parts, sub, width), bf16),
            pltpu.VMEM((n_fs, parts, sub, width), bf16),
            dma((n_fs, parts)), dma((n_fs,)), dma((full * n_tp,)), dma((full + 1,)),
            dma((n_tp,)), dma((full,)), dma((n_fs + 1, parts)),
            dma((3,)), dma((n_fs + 1, 2)), dma((1,)), dma((1,)), dma((1,)), dma((1,)),
            dma((1,)), dma((n_fs + 1,)), dma((1,)), dma((1,)), dma((2,)),
            dma((n_fs,)),
            dma((2 + parts,)), dma((6,)), dma((7 + n_fs,)),
        ],
        compiler_params=pltpu.CompilerParams(
            collective_id=0, has_side_effects=True, vmem_limit_bytes=VMEM_LIMIT
        ),
    )(
        prompt, train_gate.transpose(0, 2, 1), train_up.transpose(0, 2, 1), train_down,
        train_shared_gate.T, train_shared_up.T, train_shared_down, norm_gain[None, :],
        expert_ids.T, route_weight.T,
    )
    serve_gate, serve_up, serve_down, s_gate, s_up, s_down, mixed_out = copied(outs)
    return (
        serve_gate[None], serve_up[None], serve_down[None],
        s_gate.T, s_up.T, s_down, mixed_out.reshape(rows, width),
    )


def regroup(stacked, lowered):
    stacked = lax.all_to_all(
        lax.all_to_all(stacked, "fs", split_axis=0, concat_axis=2, tiled=True),
        "tp",
        split_axis=0,
        concat_axis=3,
        tiled=True,
    )
    lowered = lax.all_to_all(
        lax.all_to_all(lowered, "fs", split_axis=0, concat_axis=2, tiled=True),
        "tp",
        split_axis=0,
        concat_axis=1,
        tiled=True,
    )
    return (stacked, lowered)


def body(
    prompt,
    train_gate,
    train_up,
    train_down,
    train_shared_gate,
    train_shared_up,
    train_shared_down,
    norm_gain,
    expert_ids,
    route_weight,
):
    gain_col = norm_gain[:, None]
    stacked = jnp.stack((train_gate * gain_col[None], train_up * gain_col[None]), axis=1).astype(
        jnp.bfloat16
    )
    lowered = train_down.astype(jnp.bfloat16)
    stacked, lowered = regroup(stacked, lowered)
    stacked, lowered = (
        lax.all_gather(stacked, "gr", axis=2, tiled=True),
        lax.all_gather(lowered, "gr", axis=2, tiled=True),
    )
    serve_gate = stacked[:, 0]
    serve_up = stacked[:, 1]
    serve_shared_gate, serve_shared_up, serve_shared_down = (
        lax.all_gather(
            (train_shared_gate * gain_col).astype(jnp.bfloat16), ("gr", "fs"), axis=0, tiled=True
        ),
        lax.all_gather(
            (train_shared_up * gain_col).astype(jnp.bfloat16), ("gr", "fs"), axis=0, tiled=True
        ),
        lax.all_gather(train_shared_down.astype(jnp.bfloat16), ("gr", "fs"), axis=1, tiled=True),
    )
    widened = prompt.astype(jnp.float32)
    normed = (
        widened * lax.rsqrt(jnp.mean(widened * widened, axis=-1, keepdims=True) + eps_norm)
    ).astype(jnp.bfloat16)
    block_rows = lax.all_gather(normed, "tp", axis=0, tiled=True)
    gate_val = jnp.dot(block_rows, serve_shared_gate, preferred_element_type=jnp.float32)
    up_val = jnp.dot(block_rows, serve_shared_up, preferred_element_type=jnp.float32)
    shared_act = (jax.nn.silu(gate_val) * up_val).astype(jnp.bfloat16)
    shared_sum = lax.psum_scatter(
        jnp.dot(shared_act, serve_shared_down, preferred_element_type=jnp.float32).astype(
            jnp.bfloat16
        ),
        "tp",
        scatter_dimension=0,
        tiled=True,
    ).astype(jnp.float32)
    row_count = prompt.shape[0]
    top_count = expert_ids.shape[1]
    model_width = prompt.shape[1]
    expert_count = lax.axis_size("fs") * lax.axis_size("tp")
    capacity = row_count * top_count // expert_count + 1
    flat_ids = expert_ids.reshape(-1)
    onehot = (flat_ids[:, None] == jnp.arange(expert_count, dtype=jnp.int32)[None, :]).astype(
        jnp.int32
    )
    earlier = jnp.cumsum(onehot, axis=0) - onehot
    places = jnp.sum(earlier * onehot, axis=1)
    slot_ids = (flat_ids * capacity + places).reshape(row_count, top_count)
    slot_range = jnp.arange(expert_count * capacity, dtype=jnp.int32)
    dispatch = jnp.any(slot_range[:, None, None] == slot_ids[None, :, :], axis=-1).astype(
        jnp.bfloat16
    )
    outgoing = jnp.dot(dispatch, normed, preferred_element_type=jnp.float32).astype(jnp.bfloat16)
    outgoing = outgoing.reshape(expert_count, capacity, model_width)
    arrived = lax.all_to_all(outgoing, ("fs", "tp"), split_axis=0, concat_axis=0, tiled=True)
    source_count, slot_count, width_here = arrived.shape
    arrived_rows = arrived.reshape(source_count * slot_count, width_here)
    gate_val = jnp.dot(arrived_rows, serve_gate[0], preferred_element_type=jnp.float32)
    up_val = jnp.dot(arrived_rows, serve_up[0], preferred_element_type=jnp.float32)
    hidden = (jax.nn.silu(gate_val) * up_val).astype(jnp.bfloat16)
    result = jnp.dot(hidden, lowered[0], preferred_element_type=jnp.float32).astype(jnp.bfloat16)
    result = result.reshape(source_count, slot_count, width_here)
    returned = lax.all_to_all(result, ("fs", "tp"), split_axis=0, concat_axis=0, tiled=True)
    picked = returned.reshape(expert_count * capacity, model_width)[slot_ids]
    routed = jnp.sum(route_weight[:, :, None] * picked.astype(jnp.float32), axis=1)
    mixed_out = (routed + shared_sum).astype(jnp.bfloat16)
    return (
        serve_gate,
        serve_up,
        lowered,
        serve_shared_gate,
        serve_shared_up,
        serve_shared_down,
        mixed_out,
    )


def solution(mesh):
    placed = (
        P(("gr", "fs", "tp"), None),
        P(None, ("gr", "fs"), "tp"),
        P(None, ("gr", "fs"), "tp"),
        P(None, "tp", ("gr", "fs")),
        P(("gr", "fs"), "tp"),
        P(("gr", "fs"), "tp"),
        P("tp", ("gr", "fs")),
        P(("gr", "fs")),
        P(("gr", "fs", "tp"), None),
        P(("gr", "fs", "tp"), None),
    )
    n_gr, n_fs, n_tp = (mesh.shape[name] for name in ("gr", "fs", "tp"))

    def chosen(prompt, train_gate, *rest):
        rows, width = prompt.shape
        experts, cols, hid = train_gate.shape
        held = n_fs * n_tp * n_gr * CORES * 3 * hid * cols * 4 + 4 * n_fs * prompt.size * 2
        fits = n_gr == 2 and n_tp == 2 * CORES and n_fs % 2 == 0 and held < VMEM_PLAN
        even = experts == n_fs * n_tp and cols * n_gr * n_fs == width and rows == 128
        if fits and even and hid % (16 * n_fs) == 0 and cols % 128 == 0:
            return line_body(n_gr, n_fs, n_tp, prompt, train_gate, *rest)
        return body(prompt, train_gate, *rest)

    return jax.shard_map(
        chosen,
        mesh=mesh,
        in_specs=placed,
        out_specs=(
            P(("fs", "tp"), None, None),
            P(("fs", "tp"), None, None),
            P(("fs", "tp"), None, None),
            P(None, "tp"),
            P(None, "tp"),
            P("tp", None),
            P(("gr", "fs", "tp"), None),
        ),
        check_vma=False,
    )
```
